32 devices in a mesh: ep: 8 (over z, y), tp: 4 (over x, core).
Axes of the slice: x: 2, y: 2, z: 4, core: 2. Of those that a mesh axis runs over, the one named last changes fastest.
Arguments:
- mixer_input: bfloat16 [4096, 2048], P('ep'), may hold values from -6 to 6
- log_forget_total: float32 [16, 4096], P('tp'), may hold values from -684 to 0, as said below
- mixer_gain: float32 [2048], replicated, may hold values from 0.1 to 1.9
- w_query: bfloat16 [2048, 1024], P(None, 'tp'), may hold values from -1 to 1
- w_key: bfloat16 [2048, 256], P(None, 'tp'), may hold values from -8 to 8
- w_value: bfloat16 [2048, 256], P(None, 'tp'), may hold values from -0.125 to 0.125
- w_output: bfloat16 [1024, 2048], replicated, may hold values from -0.1875 to 0.1875
- mixer_post_gain: float32 [2048], replicated, may hold values from 0.1 to 1.9
- expert_input: bfloat16 [2048, 2048], P('ep'), may hold values from -6 to 6
- expert_ids: int32 [2048, 2], P('ep'), may hold values from 0 to 7, all different within a row; in each aligned block of 64 rows (0 to 63, 64 to 127, ...) at most 32 rows name the same one
- route_weight: float32 [2048, 2], P('ep'), may hold values from 0.1 to 1
- expert_gain: float32 [2048], replicated, may hold values from 0.1 to 1.9
- w_gate: bfloat16 [8, 2048, 3584], P('ep', None, 'tp'), may hold values from -0.125 to 0.125
- w_up: bfloat16 [8, 2048, 3584], P('ep', None, 'tp'), may hold values from -0.125 to 0.125
- w_down: bfloat16 [8, 3584, 2048], P('ep', 'tp'), may hold values from -0.09375 to 0.09375
- expert_post_gain: float32 [2048], replicated, may hold values from 0.1 to 1.9
Outputs:
- mixer_out: bfloat16 [4096, 2048], P(('ep', 'tp'))
- expert_out: bfloat16 [2048, 2048], P(('ep', 'tp'))
The draws below stay inside these ranges and needn't reach their ends.
Inputs may be any that keep to these rules, and one draw needn't show every extreme that they name: `expert_ids`: in each aligned block of 64 tokens no expert is named by more than 32 of them. `log_forget_total`: each head's values never rise along the positions.
All inputs are finite; a program needn't handle non-finite values.
Results may differ from the reference program's by a relative error of at most 0.012.
The reference program's roundings to bfloat16 on the way count: a program that leaves them out, or rounds other values in their place, can miss the bound.
Values may be sent and summed in bfloat16 or wider, within the bound.
A program may use at most 128 MiB of HBM per device.

```python
import math
import jax
import jax.numpy as jnp
import numpy as np
from jax import lax

D = 2048
QUERY_HEADS = 16
KV_HEADS = 4
HD = 64
FF = 3584
TOP_K = 2
ATT_ROWS = 512
ATTENTION_SPAN = 4096
MOE_TOKENS = 2048
EXPERTS = 8
QROWS = 64
CAPQ = 32
N_EP = 8
N_TP = 4


def draw_mixer_input(key, part):
    drawn = jax.random.normal(jax.random.fold_in(key, 7), (ATTENTION_SPAN, D), jnp.float32)
    return jnp.clip(drawn, -6.0, 6.0).astype(jnp.bfloat16)


def draw_log_forget_total(key, part):
    order = jax.random.permutation(jax.random.fold_in(key, 21), QUERY_HEADS)
    slow_count = QUERY_HEADS // 2
    slow = order < slow_count
    slow_rate = jax.random.uniform(jax.random.fold_in(key, 22), (QUERY_HEADS,), jnp.float32, 0.2, 0.8) / ATTENTION_SPAN
    fast_rate = 1.0 / jax.random.uniform(jax.random.fold_in(key, 23), (QUERY_HEADS,), jnp.float32, 30.0, 100.0)
    step_rate = jnp.where(slow, slow_rate, fast_rate)
    block_factor = jnp.exp(jax.random.uniform(jax.random.fold_in(key, 24), (ATTENTION_SPAN // ATT_ROWS, QUERY_HEADS), jnp.float32, math.log(0.4), math.log(2.5)))
    per_position = jnp.repeat(block_factor, ATT_ROWS, axis=0)
    rough = jax.random.uniform(jax.random.fold_in(key, 25), (ATTENTION_SPAN, QUERY_HEADS), jnp.float32, 0.3, 1.7)
    gate_logarithm = -step_rate[None, :] * per_position * rough
    spike_position = jax.random.randint(jax.random.fold_in(key, 26), (3,), 0, ATTENTION_SPAN)
    spike_length = jnp.log(jax.random.uniform(jax.random.fold_in(key, 27), (3, QUERY_HEADS), jnp.float32, 0.6, 0.8))
    match_count = (jnp.arange(ATTENTION_SPAN)[:, None] == spike_position[None, :]).astype(jnp.float32)
    gate_logarithm = gate_logarithm + jnp.sum(match_count[:, :, None] * spike_length[None, :, :], axis=1)
    return jnp.transpose(jnp.cumsum(gate_logarithm, axis=0))


def query_key_pair(key):
    query_w = jax.random.normal(jax.random.fold_in(key, 31), (D, QUERY_HEADS * HD), jnp.float32) * D ** (-0.5)
    key_w = jax.random.normal(jax.random.fold_in(key, 32), (D, KV_HEADS * HD), jnp.float32) * D ** (-0.5)
    return (jnp.clip(query_w, -1.0, 1.0), jnp.clip(key_w, -8.0, 8.0))


def draw_w_query(key, part):
    return query_key_pair(key)[0].astype(jnp.bfloat16)


def draw_w_key(key, part):
    return query_key_pair(key)[1].astype(jnp.bfloat16)


def level_of(key, extent, split, smallest, top_value):
    def one(axis_at, parts):
        heights = jax.random.uniform(jax.random.fold_in(jax.random.fold_in(key, 6), axis_at), (parts,), jnp.float32, smallest / len(split), top_value / len(split))
        return jnp.repeat(jnp.exp(heights), extent[axis_at] // parts).reshape((-1,) + (1,) * (len(extent) - axis_at - 1))

    loudness = one(*split[0])
    for cut in split[1:]:
        loudness = loudness * one(*cut)
    return loudness


def deal_out(rng, own, number, rows, number_of, top, bound, skew):
    order = jax.random.permutation(rng, number_of)
    heavy_load, usual = portions_of(number_of, rows * top, bound, skew, True), portions_of(number_of, rows * top, bound, skew, False)
    places = jnp.arange(number_of)

    def named(tallies, turn):
        used = int((tallies > 0).sum())
        fixed = max(1, used // 4)
        moved = fixed + (places - fixed + turn * (used - fixed)) % max(1, number_of - fixed)
        return jnp.zeros((number_of,), jnp.int32).at[order[jnp.where(places < fixed, places, moved)]].set(jnp.asarray(tallies, jnp.int32))

    tallies = jnp.where(number % 4 == 0, named(heavy_load, number // 4), named(usual, number - number // 4 - 1))
    mixed = jax.random.permutation(jax.random.fold_in(own, 3), number_of)
    source_of, receiver = mixed[0:number_of // 2 * 2:2], mixed[1:number_of // 2 * 2:2]
    margin = jnp.minimum(tallies[source_of] - 1, bound - tallies[receiver]) // 2
    margin = jnp.where((source_of == order[0]) | (receiver == order[0]) | (tallies[receiver] == 0), 0, jnp.maximum(margin, 0))
    moved = jax.random.randint(jax.random.fold_in(own, 4), (number_of // 2,), 0, 1 << 20) % (margin + 1)
    tallies = tallies.at[source_of].add(-moved).at[receiver].add(moved)
    items = jnp.searchsorted(jnp.cumsum(tallies), jnp.arange(rows * top), side="right").astype(jnp.int32)
    listing = items.reshape(top, rows).T
    listing = listing[jax.random.permutation(jax.random.fold_in(own, 1), rows)]
    turn = jax.random.randint(jax.random.fold_in(own, 2), (rows, 1), 0, top)
    return jnp.take_along_axis(listing, (jnp.arange(top)[None, :] + turn) % top, axis=1)


def portions_of(amount, total, reach, slope, full):
    weights = [(1 << 20) // math.isqrt(rank ** slope) + 1 for rank in range(1, amount + 1)]
    largest = reach if full else min(reach, max(-(-total // amount), total * weights[0] // sum(weights)))
    least = 1 if total - largest >= amount - 1 else 0
    counts, rest = [largest] + [least] * (amount - 1), total - largest - least * (amount - 1)
    while rest > 0:
        candidates = [i for i in range(1, amount) if counts[i] < largest] or [i for i in range(1, amount) if counts[i] < reach]
        mass, left = sum([weights[i] for i in candidates]), rest
        for i in candidates:
            addition = min(reach - counts[i], max(1, left * weights[i] // mass), rest)
            counts[i] = counts[i] + addition
            rest = rest - addition
    return np.array(counts)


def scatter_about(own_key, shape, scale, reach, split=(), held_as=jnp.bfloat16):
    gain = level_of(own_key, shape, split, -0.22, 0.18) if split else 1.0
    entries = jax.random.normal(own_key, shape, jnp.float32) * scale * gain
    return jnp.minimum(jnp.maximum(entries, -reach), reach).astype(held_as)


def setup_inputs(seed: int = 0) -> dict:
    seeds = jax.random.split(jax.random.key(seed), 17)
    mixer_input = draw_mixer_input(jax.random.fold_in(seeds[16], 71), 0)
    log_forget_total = draw_log_forget_total(jax.random.fold_in(seeds[16], 71), 0)
    mixer_gain = jnp.clip(1.0 + 0.18 * jax.random.normal(seeds[2], (D,), jnp.float32), 0.1, 1.9)
    w_query = draw_w_query(jax.random.fold_in(seeds[16], 71), 0)
    w_key = draw_w_key(jax.random.fold_in(seeds[16], 71), 0)
    w_value = scatter_about(seeds[5], (D, KV_HEADS * HD), D ** -0.5, 0.125, ((1, 4),))
    w_output = scatter_about(seeds[6], (QUERY_HEADS * HD, D), (QUERY_HEADS * HD) ** -0.5, 0.1875)
    mixer_post_gain = jnp.clip(1.0 + 0.18 * jax.random.normal(seeds[7], (D,), jnp.float32), 0.1, 1.9)
    expert_input = scatter_about(seeds[8], (MOE_TOKENS, D), 1.0, 6.0, ((0, 8),))
    expert_ids_keys = jax.random.split(jax.random.fold_in(seeds[9], 1), MOE_TOKENS // QROWS)
    expert_ids_turns = jax.random.permutation(jax.random.fold_in(seeds[9], 3), MOE_TOKENS // QROWS)
    expert_ids = jax.vmap(lambda own, number: deal_out(jax.random.fold_in(seeds[9], 2), own, number, QROWS, EXPERTS, TOP_K, CAPQ, 2))(expert_ids_keys, expert_ids_turns).reshape((MOE_TOKENS, TOP_K))
    route_weight = jnp.clip(jnp.exp(math.log(1.0) - 2.3025851 * jax.random.uniform(seeds[10], (MOE_TOKENS, TOP_K), jnp.float32) ** level_of(seeds[10], (MOE_TOKENS, TOP_K), ((0, 8),), -0.2, 0.2)), 0.1, 1.0)
    expert_gain = jnp.clip(1.0 + 0.18 * jax.random.normal(seeds[11], (D,), jnp.float32), 0.1, 1.9)
    w_gate = scatter_about(seeds[12], (EXPERTS, D, FF), D ** -0.5, 0.125, ((0, 8), (2, 4)))
    w_up = scatter_about(seeds[13], (EXPERTS, D, FF), D ** -0.5, 0.125, ((0, 8), (2, 4)))
    w_down = scatter_about(seeds[14], (EXPERTS, FF, D), FF ** -0.5, 0.09375, ((0, 8), (1, 4)))
    expert_post_gain = jnp.clip(1.0 + 0.18 * jax.random.normal(seeds[15], (D,), jnp.float32), 0.1, 1.9)
    return {"mixer_input": mixer_input, "log_forget_total": log_forget_total, "mixer_gain": mixer_gain, "w_query": w_query, "w_key": w_key, "w_value": w_value, "w_output": w_output, "mixer_post_gain": mixer_post_gain, "expert_input": expert_input, "expert_ids": expert_ids, "route_weight": route_weight, "expert_gain": expert_gain, "w_gate": w_gate, "w_up": w_up, "w_down": w_down, "expert_post_gain": expert_post_gain}


NEG_FILL = -1e+30
NORM_EPS = 1e-06

def norm_rows(values_in, gain_vec):
    widened = values_in.astype(jnp.float32)
    return widened * lax.rsqrt(lax.optimization_barrier(jnp.mean(widened * widened, axis=-1, keepdims=True)) + NORM_EPS) * gain_vec.astype(jnp.float32)

def rounded(values_in):
    return lax.optimization_barrier(values_in.astype(jnp.bfloat16))

def mixer_part(mixer_input, log_forget_total, mixer_gain, w_query, w_key, w_value, w_output, mixer_post_gain):
    normed = rounded(norm_rows(mixer_input, mixer_gain))
    queries = rounded(jnp.dot(normed, w_query, preferred_element_type=jnp.float32))
    key_rows = rounded(jnp.dot(normed, w_key, preferred_element_type=jnp.float32))
    value_rows = rounded(jnp.dot(normed, w_value, preferred_element_type=jnp.float32))
    group_size = QUERY_HEADS // KV_HEADS
    block_rows = math.gcd(ATTENTION_SPAN, 512)
    block_total = ATTENTION_SPAN // block_rows
    query_blocks = queries.reshape(block_total, block_rows, KV_HEADS, group_size, HD)
    key_wide = key_rows.astype(jnp.float32).reshape(ATTENTION_SPAN, KV_HEADS, HD)
    value_wide = value_rows.astype(jnp.float32).reshape(ATTENTION_SPAN, KV_HEADS, HD)
    gate_totals = log_forget_total.astype(jnp.float32).reshape(KV_HEADS, group_size, ATTENTION_SPAN)
    positions = jnp.arange(ATTENTION_SPAN, dtype=jnp.int32)
    score_scale = HD ** (-0.5)

    def one_block(operands):
        query_block, block_index = operands
        first_row = (block_index * block_rows).astype(jnp.int32)
        query_pos = first_row + jnp.arange(block_rows, dtype=jnp.int32)
        visible = positions[None, :] <= query_pos[:, None]
        outputs = []
        for head_group in range(KV_HEADS):
            group_gates = gate_totals[head_group]
            query_gate = lax.dynamic_slice_in_dim(group_gates, first_row, block_rows, 1)
            scores = jnp.einsum('qjd,kd->jqk', query_block[:, head_group].astype(jnp.float32), key_wide[:, head_group]) * score_scale
            scores = scores + query_gate[:, :, None] - group_gates[:, None, :]
            scores = jnp.where(visible[None], scores, NEG_FILL)
            row_max = lax.optimization_barrier(jnp.max(scores, axis=-1, keepdims=True))
            shifted = jnp.where(visible[None], jnp.exp(scores - row_max), 0.0)
            denominator = lax.optimization_barrier(jnp.sum(shifted, axis=-1))
            weights = rounded(shifted).astype(jnp.float32)
            numerator = jnp.einsum('jqk,kd->qjd', weights, value_wide[:, head_group])
            outputs.append(numerator / jnp.transpose(denominator)[:, :, None])
        return rounded(jnp.concatenate(outputs, axis=1).reshape(block_rows, QUERY_HEADS * HD))
    mixed_heads = lax.map(one_block, (query_blocks, jnp.arange(block_total, dtype=jnp.int32)))
    mixed_heads = mixed_heads.reshape(ATTENTION_SPAN, QUERY_HEADS * HD)
    projected = jnp.dot(mixed_heads, w_output, preferred_element_type=jnp.float32)
    return norm_rows(projected, mixer_post_gain).astype(jnp.bfloat16)

def expert_part(expert_input, expert_ids, route_weight, expert_gain, w_gate, w_up, w_down, expert_post_gain):
    normed = rounded(norm_rows(expert_input, expert_gain))
    assigned = MOE_TOKENS * TOP_K
    capacity = N_EP * N_TP * CAPQ
    group_units = FF // N_TP
    flat_ids = expert_ids.reshape(assigned)
    owners = jnp.concatenate([jnp.arange(assigned, dtype=jnp.int32) // TOP_K, jnp.full((1,), MOE_TOKENS, jnp.int32)])
    shares = jnp.concatenate([route_weight.reshape(assigned).astype(jnp.float32), jnp.zeros((1,), jnp.float32)])
    padded_rows = jnp.concatenate([normed, jnp.zeros((1, D), jnp.bfloat16)], axis=0)

    def one_expert(running, expert):
        chosen = flat_ids == expert
        slot_ranks = jnp.cumsum(chosen.astype(jnp.int32)) - 1
        slot_target = jnp.where(chosen, slot_ranks, capacity).astype(jnp.int32)
        slot_table = jnp.full((capacity,), assigned, jnp.int32).at[slot_target].set(jnp.arange(assigned, dtype=jnp.int32), mode='drop')
        token_rows = owners[slot_table]
        inputs = padded_rows[token_rows]
        gate_part = jnp.dot(inputs, w_gate[expert], preferred_element_type=jnp.float32)
        up_part = jnp.dot(inputs, w_up[expert], preferred_element_type=jnp.float32)
        hidden = rounded(jax.nn.silu(gate_part) * up_part)
        down_local = w_down[expert]
        summed = jnp.zeros((capacity, D), jnp.float32)
        for group_index in range(N_TP):
            low_unit = group_index * group_units
            group_term = jnp.dot(hidden[:, low_unit:low_unit + group_units], down_local[low_unit:low_unit + group_units], preferred_element_type=jnp.float32)
            summed = summed + rounded(group_term).astype(jnp.float32)
        expert_rows = rounded(summed).astype(jnp.float32)
        running = running.at[token_rows].add(shares[slot_table][:, None] * expert_rows, mode='drop')
        return (running, None)
    combined, _ = lax.scan(one_expert, jnp.zeros((MOE_TOKENS, D), jnp.float32), jnp.arange(EXPERTS, dtype=jnp.int32))
    return norm_rows(combined, expert_post_gain).astype(jnp.bfloat16)

def reference(mixer_input, log_forget_total, mixer_gain, w_query, w_key, w_value, w_output, mixer_post_gain, expert_input, expert_ids, route_weight, expert_gain, w_gate, w_up, w_down, expert_post_gain):
    mixer_out = mixer_part(mixer_input, log_forget_total, mixer_gain, w_query, w_key, w_value, w_output, mixer_post_gain)
    expert_out = expert_part(expert_input, expert_ids, route_weight, expert_gain, w_gate, w_up, w_down, expert_post_gain)
    return (mixer_out, expert_out)
```

```python
import functools

import jax
import jax.numpy as jnp
from jax import lax
from jax.experimental import pallas as pl
from jax.experimental.pallas import tpu as pltpu
from jax.sharding import PartitionSpec as P

HD = 64
TOP_K = 2
ONES = 16
LOG2E = 1.4426950408889634
NEG_FILL = -1e30
NORM_EPS = 1e-06
MESH = pl.DeviceIdType.MESH


def norm_rows(values_in, gain_vec):
    widened = values_in.astype(jnp.float32)
    return (
        widened
        * lax.rsqrt(jnp.mean(widened * widened, axis=-1, keepdims=True) + NORM_EPS)
        * gain_vec
    )


def three_pieces(wide):
    high = wide.astype(jnp.bfloat16)
    rest = wide - high.astype(jnp.float32)
    middle = rest.astype(jnp.bfloat16)
    low = (rest - middle.astype(jnp.float32)).astype(jnp.bfloat16)
    return high, middle, low


def contract(a, b, left, right):
    return lax.dot_general(
        a, b, (((left,), (right,)), ((), ())), preferred_element_type=jnp.float32
    )


def flip(place, step, size):
    total = 0
    bit = 1
    while bit < size:
        total = total + lax.rem(place // bit + step // bit, 2) * bit
        bit *= 2
    return total


def fused_kernel(
    n_ep, x_hbm, gate_ref, gain_ref, wq_hbm, wk_hbm, wv_hbm, wo_hbm, post_ref, xin_hbm,
    ids_ref, share_ref, egain_ref, wg_hbm, wu_hbm, wd_hbm, epost_ref,
    mixer_ref, expert_ref,
    x_v, wq_v, wkv_v, wo_v, xin_v, wgu_v, wd_v, out_rows, slots, product, arrived, summed,
    crossed, final, returned, weigh_v, kv_all, q_full, max_ref, acc_ref, mixed_v, heads_v,
    l_sem, ep_sem, x_sem, c_sem, d_sem, p_sem, r_sem, s_sem, b_sem, k_sem, f_sem, h_sem,
):
    own = lax.axis_index("ep")
    quarter = lax.axis_index("tp")
    across = lax.rem(quarter + 2, 4)
    beside = quarter + 1 - 2 * lax.rem(quarter, 2)
    diagonal = lax.rem(beside + 2, 4)
    column = lax.rem(own, 2)
    row = own // 2
    row_total = n_ep // 2
    partner = own + 1 - 2 * column
    heads, _, rows = q_full.shape
    token_rows = xin_v.shape[0]
    cap = out_rows.shape[1]
    width = out_rows.shape[2]
    units = wd_v.shape[0]

    def remote(source, target, sems, at_send, at_recv, axis, place):
        return pltpu.make_async_remote_copy(
            src_ref=source, dst_ref=target, send_sem=sems.at[0, at_send],
            recv_sem=sems.at[1, at_recv], device_id={axis: place}, device_id_type=MESH,
        )

    def local(index):
        pairs = (
            (xin_hbm.at[pl.ds(quarter * token_rows, token_rows)], xin_v),
            (x_hbm, x_v),
            (wk_hbm, wkv_v.at[0:HD]),
            (wv_hbm, wkv_v.at[HD : 2 * HD]),
            (wq_hbm, wq_v),
            (wg_hbm, wgu_v.at[:, 0:units]),
            (wu_hbm, wgu_v.at[:, units : 2 * units]),
            (wd_hbm, wd_v),
            (wo_hbm, wo_v),
        )
        return pltpu.make_async_copy(pairs[index][0], pairs[index][1], l_sem.at[index])

    for index in range(9):
        local(index).start()
    barrier = pltpu.get_barrier_semaphore()
    for axis, size in (("ep", n_ep), ("tp", 4)):
        place = lax.axis_index(axis)
        for step in range(1, size):
            pl.semaphore_signal(
                barrier, inc=1, device_id={axis: lax.rem(place + step, size)},
                device_id_type=MESH,
            )

    def ep_copy(source, place):
        return remote(
            out_rows.at[place], slots.at[quarter, source], ep_sem, place, source, "ep", place
        )

    def to_across(source):
        held = slots.at[quarter, source]
        return remote(held, held, x_sem, source, source, "tp", across)

    def from_across(source):
        held = slots.at[across, source]
        return remote(held, held, x_sem, source, source, "tp", across)

    def to_beside(source):
        held = slots.at[quarter, source]
        return remote(held, held, c_sem, source, source, "tp", beside)

    def from_beside(source):
        held = slots.at[beside, source]
        return remote(held, held, c_sem, source, source, "tp", beside)

    def second(source):
        held = slots.at[across, source]
        return remote(held, held, d_sem, source, source, "tp", beside)

    def from_second(source):
        held = slots.at[diagonal, source]
        return remote(held, held, d_sem, source, source, "tp", beside)

    def near(j):
        return remote(product.at[beside, j], arrived.at[0, j], p_sem, j, j, "tp", beside)

    def far(j):
        return remote(product.at[diagonal, j], arrived.at[1, j], r_sem, j, j, "tp", beside)

    def cross(j):
        return remote(summed.at[j], crossed.at[j], s_sem, j, j, "tp", across)

    def home(j, source):
        return remote(final.at[j], returned.at[source], b_sem, j, source, "ep", j)

    def chain(source, place):
        return remote(kv_all.at[source], kv_all.at[source], k_sem, source, source, "ep", place)

    def hand(source):
        return remote(kv_all.at[source], kv_all.at[source], f_sem, source, source, "ep", partner)

    def heads_copy(step):
        place = lax.rem(quarter + step, 4)
        return remote(mixed_v.at[place], heads_v.at[quarter], h_sem, step, step, "tp", place)

    def own_part(wide):
        part = 0
        for k in range(4):
            chosen = (quarter == k).astype(wide.dtype)
            part = part + wide[:, k * token_rows : (k + 1) * token_rows] * chosen
        return part

    ids = own_part(ids_ref[...])
    shares = own_part(share_ref[...])
    expert = lax.broadcasted_iota(jnp.int32, (n_ep, token_rows), 0)
    first_is = (expert == ids[0:1]).astype(jnp.float32)
    second_is = (expert == ids[1:2]).astype(jnp.float32)
    named = (first_is + second_is).astype(jnp.bfloat16)
    earlier = (
        lax.broadcasted_iota(jnp.int32, (token_rows, token_rows), 0)
        < lax.broadcasted_iota(jnp.int32, (token_rows, token_rows), 1)
    ).astype(jnp.bfloat16)
    before = jnp.dot(named, earlier, preferred_element_type=jnp.float32).astype(jnp.bfloat16)
    total = n_ep * cap
    at_row = lax.broadcasted_iota(jnp.int32, (total, n_ep), 0)
    low_row = lax.broadcasted_iota(jnp.int32, (total, n_ep), 1) * cap
    spread = ((at_row >= low_row) & (at_row < low_row + cap)).astype(jnp.bfloat16)
    rank = (lax.broadcasted_iota(jnp.int32, (total, token_rows), 0) & (cap - 1)).astype(
        jnp.float32
    )
    here = jnp.dot(spread, before, preferred_element_type=jnp.float32) == rank
    sel = jnp.where(here, jnp.dot(spread, named, preferred_element_type=jnp.float32), 0.0)
    local(0).wait()
    normed_m = norm_rows(xin_v[...], egain_ref[...]).astype(jnp.bfloat16)
    outgoing = jnp.dot(sel.astype(jnp.bfloat16), normed_m, preferred_element_type=jnp.float32)
    out_rows[...] = outgoing.astype(jnp.bfloat16).reshape(out_rows.shape)
    slots[quarter, own] = out_rows[own]
    pl.semaphore_wait(barrier, n_ep - 1 + 3)
    for step in range(1, 4):
        ep_copy(own, flip(own, step, n_ep)).start()
    to_across(own).start()
    to_beside(own).start()

    local(1).wait()
    slab = min(64, rows)

    def norm_slab(index, carry):
        at = pl.ds(pl.multiple_of(index * slab, slab), slab)
        x_v[at] = norm_rows(x_v[at], gain_ref[...]).astype(jnp.bfloat16)
        return carry

    lax.fori_loop(0, rows // slab, norm_slab, 0)
    local(2).wait()
    local(3).wait()
    kv_all[own] = contract(x_v[...], wkv_v[...], 1, 1).astype(jnp.bfloat16)

    @pl.when(row + 1 < row_total)
    def _():
        chain(own, own + 2).start()

    @pl.when(column == 0)
    def _():
        hand(own).start()

    local(4).wait()
    queries = jnp.dot(x_v[...], wq_v[...], preferred_element_type=jnp.float32)
    queries = queries.astype(jnp.bfloat16).astype(jnp.float32).T * (LOG2E * HD ** (-0.5))
    piece_row = lax.broadcasted_iota(jnp.int32, (HD, rows), 0)
    for head in range(heads):
        wide = queries[head * HD : (head + 1) * HD]
        high = wide.astype(jnp.bfloat16)
        q_full[head, 0:HD] = high
        q_full[head, HD : 2 * HD] = jnp.zeros((HD, rows), jnp.bfloat16)
        q_full[head, 2 * HD : 3 * HD] = (wide - high.astype(jnp.float32)).astype(jnp.bfloat16)
        ones = (piece_row == head) | (piece_row == heads + head) | (piece_row == 2 * heads + head)
        q_full[head, 3 * HD : 4 * HD] = ones.astype(jnp.bfloat16)

    low_lane = lax.broadcasted_iota(jnp.int32, (n_ep, total), 0) * cap
    at_lane = lax.broadcasted_iota(jnp.int32, (n_ep, total), 1)
    spread_t = ((at_lane >= low_lane) & (at_lane < low_lane + cap)).astype(jnp.bfloat16)
    rank_t = (lax.broadcasted_iota(jnp.int32, (token_rows, total), 1) & (cap - 1)).astype(
        jnp.float32
    )
    here_t = contract(before, spread_t, 0, 0) == rank_t
    weighed = first_is * shares[0:1] + second_is * shares[1:2]
    for index, piece in enumerate(three_pieces(weighed)):
        placed = jnp.where(here_t, contract(piece, spread_t, 0, 0), 0.0)
        weigh_v[index * token_rows : (index + 1) * token_rows] = placed.astype(jnp.bfloat16)

    max_ref[...] = jnp.full(max_ref.shape, NEG_FILL, jnp.float32)
    acc_ref[...] = jnp.zeros(acc_ref.shape, jnp.float32)

    def attend(index, diag):
        kv = kv_all[index]
        first = pl.multiple_of(index * rows, rows)
        pieces = three_pieces(gate_ref[:, pl.ds(first, rows)] * (-LOG2E))
        pieces = [piece.astype(jnp.float32) for piece in pieces]
        stacked = jnp.concatenate(
            [jnp.zeros((HD, rows), jnp.float32)]
            + pieces
            + [jnp.zeros((HD - 3 * heads, rows), jnp.float32)],
            axis=0,
        )
        lane = lax.broadcasted_iota(jnp.int32, kv.shape, 1)
        gated = jnp.where(lane < HD, kv, stacked.T.astype(jnp.bfloat16))
        keys = jnp.concatenate([kv, gated], axis=1)
        values = kv.T
        at = lax.broadcasted_iota(jnp.int32, values.shape, 0)
        values = jnp.where(at < HD, jnp.ones_like(values), values)[HD - ONES :]
        for head in range(heads):
            scores = jnp.dot(keys, q_full[head], preferred_element_type=jnp.float32)
            if diag:
                key = lax.broadcasted_iota(jnp.int32, scores.shape, 0)
                query = lax.broadcasted_iota(jnp.int32, scores.shape, 1)
                scores = jnp.where(key <= query, scores, NEG_FILL)
            old_max = max_ref[head]
            new_max = jnp.maximum(old_max, jnp.max(scores, axis=0, keepdims=True))
            shifted = jnp.exp2(scores - new_max).astype(jnp.bfloat16)
            acc_ref[head] = acc_ref[head] * jnp.exp2(old_max - new_max) + jnp.dot(
                values, shifted, preferred_element_type=jnp.float32
            )
            max_ref[head] = new_max

    attend(own, True)
    for index in (5, 6, 7):
        local(index).wait()

    def block_of(t):
        return own + lax.rem(t, 2) * (partner - own) - 2 * (t // 2)

    def run(t, carry):
        @pl.when(t + 4 < n_ep)
        def _():
            ep_copy(own, flip(own, t + 4, n_ep)).start()

        @pl.when((t > 0) & (t < n_ep))
        def _():
            source = flip(own, t, n_ep)
            ep_copy(source, source).wait_recv()
            to_across(source).start()
            to_beside(source).start()

        @pl.when((t > 0) & (lax.rem(t, 2) == 0) & (t // 2 <= row))
        def _():
            source = own - t
            chain(source, own).wait_recv()
            hand(source).start()

            @pl.when(row + 1 < row_total)
            def _():
                chain(source, own + 2).start()

        @pl.when((t >= 1) & (t <= n_ep))
        def _():
            source = flip(own, t - 1, n_ep)
            from_across(source).wait_recv()
            second(source).start()

        @pl.when(t >= 4)
        def _():
            j = flip(own, t - 4, n_ep)
            near(j).wait_recv()
            cross(j).wait_recv()
            whole = product[quarter, j].astype(jnp.float32) + arrived[0, j].astype(jnp.float32)
            final[j] = (whole + crossed[j].astype(jnp.float32)).astype(jnp.bfloat16)

            @pl.when(t > 4)
            def _():
                home(j, own).start()

        @pl.when((t >= 3) & (t < n_ep + 3))
        def _():
            j = flip(own, t - 3, n_ep)
            far(j).wait_recv()
            pair = product[across, j].astype(jnp.float32) + arrived[1, j].astype(jnp.float32)
            summed[j] = pair.astype(jnp.bfloat16)
            cross(j).start()

        @pl.when((t >= 2) & (t < n_ep + 2))
        def _():
            source = flip(own, t - 2, n_ep)
            from_beside(source).wait_recv()
            from_second(source).wait_recv()
            tokens = slots[:, source].reshape(4 * cap, width)
            both = jnp.dot(tokens, wgu_v[...], preferred_element_type=jnp.float32)
            gate_part = both[:, :units]
            hidden = gate_part / (1.0 + jnp.exp(-gate_part)) * both[:, units:]
            terms = jnp.dot(
                hidden.astype(jnp.bfloat16), wd_v[...], preferred_element_type=jnp.float32
            )
            product[:, source] = terms.astype(jnp.bfloat16).reshape(4, cap, width)
            far(source).start()
            near(source).start()

        @pl.when((t >= 2) & (t <= n_ep))
        def _():
            turn = t - 1

            @pl.when((turn // 2 <= row) & ((turn > 1) | (column == 1)))
            def _():
                block = block_of(turn)

                @pl.when(lax.rem(turn, 2) == 1)
                def _():
                    hand(block).wait_recv()

                attend(block, False)

        @pl.when(t == n_ep + 1)
        def _():
            parts = [acc_ref[head, ONES:] / acc_ref[head, 0:1] for head in range(heads)]
            mixed = jnp.concatenate(parts, axis=0).T.astype(jnp.bfloat16)
            mixed_v[...] = mixed.reshape(mixed_v.shape)
            for step in range(1, 4):
                heads_copy(step).start()
            heads_v[quarter] = mixed_v[quarter]

        return carry

    lax.fori_loop(0, n_ep + 4, run, 0)
    returned[own] = final[own]

    for step in range(1, 4):
        heads_copy(step).wait()
    local(8).wait()
    by_rows = jnp.concatenate([heads_v[k] for k in range(4)], axis=1)
    projected = jnp.dot(by_rows, wo_v[...], preferred_element_type=jnp.float32)
    mixer_ref[...] = norm_rows(projected, post_ref[...]).astype(jnp.bfloat16)

    def come_home(step, carry):
        j = flip(own, step, n_ep)
        home(j, j).wait_recv()
        return carry

    lax.fori_loop(1, n_ep, come_home, 0)
    rows_back = returned[...].reshape(total, width)
    picked = jnp.dot(weigh_v[...], rows_back, preferred_element_type=jnp.float32)
    combined = picked[:token_rows] + picked[token_rows : 2 * token_rows]
    combined = combined + picked[2 * token_rows :]
    expert_ref[...] = norm_rows(combined, epost_ref[...]).astype(jnp.bfloat16)

    def drain(step, carry):
        j = flip(own, step, n_ep)
        to_across(j).wait_send()
        to_beside(j).wait_send()
        second(j).wait_send()
        near(j).wait_send()
        far(j).wait_send()
        cross(j).wait_send()

        @pl.when(step > 0)
        def _():
            ep_copy(own, j).wait_send()
            home(j, own).wait_send()

        return carry

    lax.fori_loop(0, n_ep, drain, 0)

    def drain_kv(step, carry):
        source = own - 2 * step

        @pl.when((step <= row) & (row + 1 < row_total))
        def _():
            chain(source, own + 2).wait_send()

        @pl.when((step <= row) & ((step > 0) | (column == 0)))
        def _():
            hand(source).wait_send()

        return carry

    lax.fori_loop(0, row_total, drain_kv, 0)


def per_device(
    mixer_input, log_forget_total, mixer_gain, w_query, w_key, w_value, w_output,
    mixer_post_gain, expert_input, expert_ids, route_weight, expert_gain, w_gate, w_up,
    w_down, expert_post_gain,
):
    n_ep = lax.axis_size("ep")
    rows, width = mixer_input.shape
    head_columns = w_query.shape[1]
    heads = head_columns // HD
    token_rows = expert_input.shape[0] // 4
    cap = 2 * TOP_K * token_rows // n_ep
    units = w_gate.shape[2]
    out_columns = w_output.shape[0]
    half = jnp.bfloat16
    chunk = (n_ep, cap, width)
    pair = pltpu.SemaphoreType.DMA((2, n_ep))
    vmem = pl.BlockSpec(memory_space=pltpu.VMEM)
    anywhere = pl.BlockSpec(memory_space=pl.ANY)
    scratch = [
        pltpu.VMEM((rows, width), half),
        pltpu.VMEM((width, head_columns), half),
        pltpu.VMEM((2 * HD, width), half),
        pltpu.VMEM((out_columns, width), half),
        pltpu.VMEM((token_rows, width), half),
        pltpu.VMEM((width, 2 * units), half),
        pltpu.VMEM((units, width), half),
        pltpu.VMEM(chunk, half),
        pltpu.VMEM((4,) + chunk, half),
        pltpu.VMEM((4,) + chunk, half),
        pltpu.VMEM((2,) + chunk, half),
        pltpu.VMEM(chunk, half),
        pltpu.VMEM(chunk, half),
        pltpu.VMEM(chunk, half),
        pltpu.VMEM(chunk, half),
        pltpu.VMEM((3 * token_rows, n_ep * cap), half),
        pltpu.VMEM((n_ep, rows, 2 * HD), half),
        pltpu.VMEM((heads, 4 * HD, rows), half),
        pltpu.VMEM((heads, 1, rows), jnp.float32),
        pltpu.VMEM((heads, HD + ONES, rows), jnp.float32),
        pltpu.VMEM((4, rows // 4, head_columns), half),
        pltpu.VMEM((4, rows // 4, head_columns), half),
        pltpu.SemaphoreType.DMA((9,)),
    ] + [pair] * 10 + [pltpu.SemaphoreType.DMA((2, 4))]
    return pl.pallas_call(
        functools.partial(fused_kernel, n_ep),
        out_shape=(
            jax.ShapeDtypeStruct((rows // 4, width), half),
            jax.ShapeDtypeStruct((token_rows, width), half),
        ),
        in_specs=[
            anywhere, vmem, vmem, anywhere, anywhere, anywhere, anywhere, vmem, anywhere,
            vmem, vmem, vmem, anywhere, anywhere, anywhere, vmem,
        ],
        out_specs=(vmem, vmem),
        scratch_shapes=scratch,
        compiler_params=pltpu.CompilerParams(
            collective_id=0, has_side_effects=True, vmem_limit_bytes=60 * 1024 * 1024
        ),
        name="fused",
    )(
        mixer_input, log_forget_total, mixer_gain[None], w_query, w_key.T, w_value.T, w_output,
        mixer_post_gain[None], expert_input, expert_ids.T, route_weight.T, expert_gain[None],
        w_gate[0], w_up[0], w_down[0], expert_post_gain[None],
    )


def solution(mesh):
    placed = (
        P("ep", None),
        P("tp", None),
        P(),
        P(None, "tp"),
        P(None, "tp"),
        P(None, "tp"),
        P(),
        P(),
        P("ep", None),
        P("ep", None),
        P("ep", None),
        P(),
        P("ep", None, "tp"),
        P("ep", None, "tp"),
        P("ep", "tp", None),
        P(),
    )
    return jax.shard_map(
        per_device,
        mesh=mesh,
        in_specs=placed,
        out_specs=(P(("ep", "tp"), None), P(("ep", "tp"), None)),
        check_vma=False,
    )
```

```python
import functools

import jax
import jax.numpy as jnp
from jax import lax
from jax.experimental import pallas as pl
from jax.experimental.pallas import tpu as pltpu
from jax.sharding import PartitionSpec as P

HD = 64
TOP_K = 2
ONES = 16
LOG2E = 1.4426950408889634
NEG_FILL = -1e30
NORM_EPS = 1e-06
MESH = pl.DeviceIdType.MESH
SOON = 5
LATER = 8


def norm_rows(values_in, gain_vec):
    widened = values_in.astype(jnp.float32)
    return (
        widened
        * lax.rsqrt(jnp.mean(widened * widened, axis=-1, keepdims=True) + NORM_EPS)
        * gain_vec
    )


def three_pieces(wide):
    high = wide.astype(jnp.bfloat16)
    rest = wide - high.astype(jnp.float32)
    middle = rest.astype(jnp.bfloat16)
    low = (rest - middle.astype(jnp.float32)).astype(jnp.bfloat16)
    return high, middle, low


def contract(a, b, left, right):
    return lax.dot_general(
        a, b, (((left,), (right,)), ((), ())), preferred_element_type=jnp.float32
    )


def flip(place, step, size):
    total = 0
    bit = 1
    while bit < size:
        total = total + lax.rem(place // bit + step // bit, 2) * bit
        bit *= 2
    return total


def fused_kernel(
    n_ep, x_hbm, gate_hbm, gain_hbm, wq_hbm, wk_hbm, wv_hbm, wo_hbm, post_hbm, xin_hbm,
    ids_hbm, share_hbm, egain_hbm, wg_hbm, wu_hbm, wd_hbm, epost_hbm,
    mixer_ref, expert_ref,
    gate_ref, gain_ref, post_ref, ids_ref, share_ref, egain_ref, epost_ref, x_v, wq_v, wkv_v, wo_v, xin_v, wgu_v, wd_v, out_rows, slots, product, arrived, summed,
    crossed, final, returned, weigh_v, kv_all, q_full, max_ref, acc_ref, mixed_v, heads_v,
    l_sem, ep_sem, x_sem, c_sem, d_sem, p_sem, r_sem, s_sem, b_sem, k_sem, f_sem, h_sem,
):
    own = lax.axis_index("ep")
    quarter = lax.axis_index("tp")
    across = lax.rem(quarter + 2, 4)
    beside = quarter + 1 - 2 * lax.rem(quarter, 2)
    diagonal = lax.rem(beside + 2, 4)
    column = lax.rem(own, 2)
    row = own // 2
    row_total = n_ep // 2
    partner = own + 1 - 2 * column
    heads, _, rows = q_full.shape
    token_rows = xin_v.shape[0]
    cap = out_rows.shape[1]
    width = out_rows.shape[2]
    units = wd_v.shape[0]

    def remote(source, target, sems, at_send, at_recv, axis, place):
        return pltpu.make_async_remote_copy(
            src_ref=source, dst_ref=target, send_sem=sems.at[0, at_send],
            recv_sem=sems.at[1, at_recv], device_id={axis: place}, device_id_type=MESH,
        )

    def local(index):
        pairs = (
            (ids_hbm, ids_ref),
            (xin_hbm.at[pl.ds(quarter * token_rows, token_rows)], xin_v),
            (egain_hbm, egain_ref),
            (share_hbm, share_ref),
            (x_hbm, x_v),
            (gain_hbm, gain_ref),
            (wk_hbm, wkv_v.at[0:HD]),
            (wv_hbm, wkv_v.at[HD : 2 * HD]),
            (wq_hbm, wq_v),
            (gate_hbm, gate_ref),
            (wg_hbm, wgu_v.at[:, 0:units]),
            (wu_hbm, wgu_v.at[:, units : 2 * units]),
            (wd_hbm, wd_v),
            (wo_hbm, wo_v),
            (post_hbm, post_ref),
            (epost_hbm, epost_ref),
        )
        return pltpu.make_async_copy(pairs[index][0], pairs[index][1], l_sem.at[index])

    for index in range(16):
        local(index).start()
    barrier = pltpu.get_barrier_semaphore()
    for axis, size in (("ep", n_ep), ("tp", 4)):
        place = lax.axis_index(axis)
        for step in range(1, size):
            pl.semaphore_signal(
                barrier, inc=1, device_id={axis: lax.rem(place + step, size)},
                device_id_type=MESH,
            )

    def ep_copy(source, place):
        return remote(
            out_rows.at[place], slots.at[quarter, source], ep_sem, place, source, "ep", place
        )

    def to_across(source):
        held = slots.at[quarter, source]
        return remote(held, held, x_sem, source, source, "tp", across)

    def from_across(source):
        held = slots.at[across, source]
        return remote(held, held, x_sem, source, source, "tp", across)

    def to_beside(source):
        held = slots.at[quarter, source]
        return remote(held, held, c_sem, source, source, "tp", beside)

    def from_beside(source):
        held = slots.at[beside, source]
        return remote(held, held, c_sem, source, source, "tp", beside)

    def second(source):
        held = slots.at[across, source]
        return remote(held, held, d_sem, source, source, "tp", beside)

    def from_second(source):
        held = slots.at[diagonal, source]
        return remote(held, held, d_sem, source, source, "tp", beside)

    def near(j):
        return remote(product.at[beside, j], arrived.at[0, j], p_sem, j, j, "tp", beside)

    def far(j):
        return remote(product.at[diagonal, j], arrived.at[1, j], r_sem, j, j, "tp", beside)

    def cross(j):
        return remote(summed.at[j], crossed.at[j], s_sem, j, j, "tp", across)

    def home(j, source):
        return remote(final.at[j], returned.at[source], b_sem, j, source, "ep", j)

    def chain(source, place):
        return remote(kv_all.at[source], kv_all.at[source], k_sem, source, source, "ep", place)

    def hand(source):
        return remote(kv_all.at[source], kv_all.at[source], f_sem, source, source, "ep", partner)

    def heads_copy(step):
        place = lax.rem(quarter + step, 4)
        return remote(mixed_v.at[place], heads_v.at[quarter], h_sem, step, step, "tp", place)

    def peer(step):
        return flip(own, step, n_ep)

    def own_part(wide):
        part = 0
        for k in range(4):
            chosen = (quarter == k).astype(wide.dtype)
            part = part + wide[:, k * token_rows : (k + 1) * token_rows] * chosen
        return part

    local(0).wait()
    ids = own_part(ids_ref[...])
    expert = lax.broadcasted_iota(jnp.int32, (n_ep, token_rows), 0)
    first_is = (expert == ids[0:1]).astype(jnp.float32)
    second_is = (expert == ids[1:2]).astype(jnp.float32)
    named = (first_is + second_is).astype(jnp.bfloat16)
    earlier = (
        lax.broadcasted_iota(jnp.int32, (token_rows, token_rows), 0)
        < lax.broadcasted_iota(jnp.int32, (token_rows, token_rows), 1)
    ).astype(jnp.bfloat16)
    before = jnp.dot(named, earlier, preferred_element_type=jnp.float32).astype(jnp.bfloat16)
    total = n_ep * cap
    at_row = lax.broadcasted_iota(jnp.int32, (total, n_ep), 0)
    low_row = lax.broadcasted_iota(jnp.int32, (total, n_ep), 1) * cap
    spread = ((at_row >= low_row) & (at_row < low_row + cap)).astype(jnp.bfloat16)
    rank = (lax.broadcasted_iota(jnp.int32, (total, token_rows), 0) & (cap - 1)).astype(
        jnp.float32
    )
    here = jnp.dot(spread, before, preferred_element_type=jnp.float32) == rank
    sel = jnp.where(here, jnp.dot(spread, named, preferred_element_type=jnp.float32), 0.0)
    local(1).wait()
    local(2).wait()
    normed_m = norm_rows(xin_v[...], egain_ref[...]).astype(jnp.bfloat16)
    outgoing = jnp.dot(sel.astype(jnp.bfloat16), normed_m, preferred_element_type=jnp.float32)
    out_rows[...] = outgoing.astype(jnp.bfloat16).reshape(out_rows.shape)
    slots[quarter, own] = out_rows[own]
    pl.semaphore_wait(barrier, n_ep - 1 + 3)
    for step in range(1, SOON):
        ep_copy(own, peer(step)).start()
    to_across(own).start()
    to_beside(own).start()

    local(4).wait()
    local(5).wait()
    slab = min(64, rows)

    def norm_slab(index, carry):
        at = pl.ds(pl.multiple_of(index * slab, slab), slab)
        x_v[at] = norm_rows(x_v[at], gain_ref[...]).astype(jnp.bfloat16)
        return carry

    lax.fori_loop(0, rows // slab, norm_slab, 0)
    local(6).wait()
    local(7).wait()
    kv_all[own] = contract(x_v[...], wkv_v[...], 1, 1).astype(jnp.bfloat16)

    @pl.when(row + 1 < row_total)
    def _():
        chain(own, own + 2).start()

    @pl.when(column == 0)
    def _():
        hand(own).start()

    def send_rest(step, carry):
        ep_copy(own, peer(step)).start()
        return carry

    lax.fori_loop(SOON, n_ep, send_rest, 0)
    local(8).wait()
    queries = jnp.dot(x_v[...], wq_v[...], preferred_element_type=jnp.float32)
    queries = queries.astype(jnp.bfloat16).astype(jnp.float32).T * (LOG2E * HD ** (-0.5))
    piece_row = lax.broadcasted_iota(jnp.int32, (HD, rows), 0)
    for head in range(heads):
        wide = queries[head * HD : (head + 1) * HD]
        high = wide.astype(jnp.bfloat16)
        q_full[head, 0:HD] = high
        q_full[head, HD : 2 * HD] = jnp.zeros((HD, rows), jnp.bfloat16)
        q_full[head, 2 * HD : 3 * HD] = (wide - high.astype(jnp.float32)).astype(jnp.bfloat16)
        ones = (piece_row == head) | (piece_row == heads + head) | (piece_row == 2 * heads + head)
        q_full[head, 3 * HD : 4 * HD] = ones.astype(jnp.bfloat16)

    low_lane = lax.broadcasted_iota(jnp.int32, (n_ep, total), 0) * cap
    at_lane = lax.broadcasted_iota(jnp.int32, (n_ep, total), 1)
    spread_t = ((at_lane >= low_lane) & (at_lane < low_lane + cap)).astype(jnp.bfloat16)
    rank_t = (lax.broadcasted_iota(jnp.int32, (token_rows, total), 1) & (cap - 1)).astype(
        jnp.float32
    )
    here_t = contract(before, spread_t, 0, 0) == rank_t
    local(3).wait()
    shares = own_part(share_ref[...])
    weighed = first_is * shares[0:1] + second_is * shares[1:2]
    for index, piece in enumerate(three_pieces(weighed)):
        placed = jnp.where(here_t, contract(piece, spread_t, 0, 0), 0.0)
        weigh_v[index * token_rows : (index + 1) * token_rows] = placed.astype(jnp.bfloat16)

    max_ref[...] = jnp.full(max_ref.shape, NEG_FILL, jnp.float32)
    acc_ref[...] = jnp.zeros(acc_ref.shape, jnp.float32)

    def attend(index, diag):
        kv = kv_all[index]
        first = pl.multiple_of(index * rows, rows)
        pieces = three_pieces(gate_ref[:, pl.ds(first, rows)] * (-LOG2E))
        pieces = [piece.astype(jnp.float32) for piece in pieces]
        stacked = jnp.concatenate(
            [jnp.zeros((HD, rows), jnp.float32)]
            + pieces
            + [jnp.zeros((HD - 3 * heads, rows), jnp.float32)],
            axis=0,
        )
        lane = lax.broadcasted_iota(jnp.int32, kv.shape, 1)
        gated = jnp.where(lane < HD, kv, stacked.T.astype(jnp.bfloat16))
        keys = jnp.concatenate([kv, gated], axis=1)
        values = kv.T
        at = lax.broadcasted_iota(jnp.int32, values.shape, 0)
        values = jnp.where(at < HD, jnp.ones_like(values), values)[HD - ONES :]
        for head in range(heads):
            scores = jnp.dot(keys, q_full[head], preferred_element_type=jnp.float32)
            if diag:
                key = lax.broadcasted_iota(jnp.int32, scores.shape, 0)
                query = lax.broadcasted_iota(jnp.int32, scores.shape, 1)
                scores = jnp.where(key <= query, scores, NEG_FILL)
            old_max = max_ref[head]
            new_max = jnp.maximum(old_max, jnp.max(scores, axis=0, keepdims=True))
            shifted = jnp.exp2(scores - new_max).astype(jnp.bfloat16)
            acc_ref[head] = acc_ref[head] * jnp.exp2(old_max - new_max) + jnp.dot(
                values, shifted, preferred_element_type=jnp.float32
            )
            max_ref[head] = new_max

    for index in (9, 10, 11, 12):
        local(index).wait()

    def block_of(t):
        return own + lax.rem(t, 2) * (partner - own) - 2 * (t // 2)

    def pass_across(step):
        j = peer(step)
        far(j).wait_recv()
        pair = product[across, j].astype(jnp.float32) + arrived[1, j].astype(jnp.float32)
        summed[j] = pair.astype(jnp.bfloat16)
        cross(j).start()

    def finish(step):
        j = peer(step)
        near(j).wait_recv()
        cross(j).wait_recv()
        whole = product[quarter, j].astype(jnp.float32) + arrived[0, j].astype(jnp.float32)
        final[j] = (whole + crossed[j].astype(jnp.float32)).astype(jnp.bfloat16)

        @pl.when(step > 0)
        def _():
            home(j, own).start()

    half = n_ep // 2

    def by_urgency(step, task):
        @pl.when((step >= half) & (step < n_ep))
        def _():
            task(step)

        near_step = step - half + 1 - 0

        @pl.when((near_step >= 1) & (near_step < half))
        def _():
            task(near_step)

        @pl.when(step == n_ep)
        def _():
            task(0)

    def run(t, carry):
        @pl.when((t > 0) & (t < n_ep))
        def _():
            source = peer(t)
            ep_copy(source, source).wait_recv()
            to_across(source).start()
            to_beside(source).start()

        early = t - LATER + 2

        @pl.when((early > 0) & (lax.rem(early + n_ep, 2) == 0) & (early <= 2 * row))
        def _():
            source = own - early
            chain(source, own).wait_recv()
            hand(source).start()

            @pl.when(row + 1 < row_total)
            def _():
                chain(source, own + 2).start()

        @pl.when((t >= 2) & (t < n_ep + 2))
        def _():
            source = peer(t - 2)
            from_across(source).wait_recv()
            second(source).start()

        by_urgency(t - 4, pass_across)

        @pl.when((t >= 3) & (t < n_ep + 3))
        def _():
            source = peer(t - 3)
            from_beside(source).wait_recv()
            from_second(source).wait_recv()
            tokens = slots[:, source].reshape(4 * cap, width)
            both = jnp.dot(tokens, wgu_v[...], preferred_element_type=jnp.float32)
            gate_part = both[:, :units]
            hidden = gate_part / (1.0 + jnp.exp(-gate_part)) * both[:, units:]
            terms = jnp.dot(
                hidden.astype(jnp.bfloat16), wd_v[...], preferred_element_type=jnp.float32
            )
            product[:, source] = terms.astype(jnp.bfloat16).reshape(4, cap, width)
            far(source).start()
            near(source).start()

        @pl.when(t == 2)
        def _():
            attend(own, True)

        @pl.when((t > LATER) & (t < n_ep + LATER))
        def _():
            turn = t - LATER

            @pl.when((turn // 2 <= row) & ((turn > 1) | (column == 1)))
            def _():
                block = block_of(turn)

                @pl.when(lax.rem(turn, 2) == 1)
                def _():
                    hand(block).wait_recv()

                attend(block, False)

        by_urgency(t - 5, finish)

        done = t - LATER - 2 * row

        @pl.when(done == 1)
        def _():
            parts = [acc_ref[head, ONES:] / acc_ref[head, 0:1] for head in range(heads)]
            mixed = jnp.concatenate(parts, axis=0).T.astype(jnp.bfloat16)
            mixed_v[...] = mixed.reshape(mixed_v.shape)
            for step in range(1, 4):
                heads_copy(step).start()
            heads_v[quarter] = mixed_v[quarter]

        @pl.when(t == n_ep + LATER)
        def _():
            for step in range(1, 4):
                heads_copy(step).wait()
            local(13).wait()
            local(14).wait()
            by_rows = jnp.concatenate([heads_v[k] for k in range(4)], axis=1)
            projected = jnp.dot(by_rows, wo_v[...], preferred_element_type=jnp.float32)
            mixer_ref[...] = norm_rows(projected, post_ref[...]).astype(jnp.bfloat16)

        return carry

    lax.fori_loop(0, n_ep + max(LATER + 1, 5 + 1), run, 0)
    returned[own] = final[own]

    def come_home(step, carry):
        j = flip(own, step, n_ep)
        home(j, j).wait_recv()
        return carry

    lax.fori_loop(1, n_ep, come_home, 0)
    local(15).wait()
    rows_back = returned[...].reshape(total, width)
    picked = jnp.dot(weigh_v[...], rows_back, preferred_element_type=jnp.float32)
    combined = picked[:token_rows] + picked[token_rows : 2 * token_rows]
    combined = combined + picked[2 * token_rows :]
    expert_ref[...] = norm_rows(combined, epost_ref[...]).astype(jnp.bfloat16)

    def drain(step, carry):
        j = flip(own, step, n_ep)
        to_across(j).wait_send()
        to_beside(j).wait_send()
        second(j).wait_send()
        near(j).wait_send()
        far(j).wait_send()
        cross(j).wait_send()

        @pl.when(step > 0)
        def _():
            ep_copy(own, j).wait_send()
            home(j, own).wait_send()

        return carry

    lax.fori_loop(0, n_ep, drain, 0)

    def drain_kv(step, carry):
        source = own - 2 * step

        @pl.when((step <= row) & (row + 1 < row_total))
        def _():
            chain(source, own + 2).wait_send()

        @pl.when((step <= row) & ((step > 0) | (column == 0)))
        def _():
            hand(source).wait_send()

        return carry

    lax.fori_loop(0, row_total, drain_kv, 0)


def per_device(
    mixer_input, log_forget_total, mixer_gain, w_query, w_key, w_value, w_output,
    mixer_post_gain, expert_input, expert_ids, route_weight, expert_gain, w_gate, w_up,
    w_down, expert_post_gain,
):
    n_ep = lax.axis_size("ep")
    rows, width = mixer_input.shape
    head_columns = w_query.shape[1]
    heads = head_columns // HD
    token_rows = expert_input.shape[0] // 4
    cap = 2 * TOP_K * token_rows // n_ep
    units = w_gate.shape[2]
    out_columns = w_output.shape[0]
    half = jnp.bfloat16
    chunk = (n_ep, cap, width)
    pair = pltpu.SemaphoreType.DMA((2, n_ep))
    vmem = pl.BlockSpec(memory_space=pltpu.VMEM)
    far_memory = pl.BlockSpec(memory_space=pltpu.HBM)
    gains = pltpu.VMEM((1, width), jnp.float32)
    scratch = [
        pltpu.VMEM(log_forget_total.shape, jnp.float32),
        gains,
        gains,
        pltpu.VMEM((TOP_K, 4 * token_rows), jnp.int32),
        pltpu.VMEM((TOP_K, 4 * token_rows), jnp.float32),
        gains,
        gains,
        pltpu.VMEM((rows, width), half),
        pltpu.VMEM((width, head_columns), half),
        pltpu.VMEM((2 * HD, width), half),
        pltpu.VMEM((out_columns, width), half),
        pltpu.VMEM((token_rows, width), half),
        pltpu.VMEM((width, 2 * units), half),
        pltpu.VMEM((units, width), half),
        pltpu.VMEM(chunk, half),
        pltpu.VMEM((4,) + chunk, half),
        pltpu.VMEM((4,) + chunk, half),
        pltpu.VMEM((2,) + chunk, half),
        pltpu.VMEM(chunk, half),
        pltpu.VMEM(chunk, half),
        pltpu.VMEM(chunk, half),
        pltpu.VMEM(chunk, half),
        pltpu.VMEM((3 * token_rows, n_ep * cap), half),
        pltpu.VMEM((n_ep, rows, 2 * HD), half),
        pltpu.VMEM((heads, 4 * HD, rows), half),
        pltpu.VMEM((heads, 1, rows), jnp.float32),
        pltpu.VMEM((heads, HD + ONES, rows), jnp.float32),
        pltpu.VMEM((4, rows // 4, head_columns), half),
        pltpu.VMEM((4, rows // 4, head_columns), half),
        pltpu.SemaphoreType.DMA((16,)),
    ] + [pair] * 10 + [pltpu.SemaphoreType.DMA((2, 4))]
    return pl.pallas_call(
        functools.partial(fused_kernel, n_ep),
        out_shape=(
            jax.ShapeDtypeStruct((rows // 4, width), half),
            jax.ShapeDtypeStruct((token_rows, width), half),
        ),
        in_specs=[far_memory] * 16,
        out_specs=(vmem, vmem),
        scratch_shapes=scratch,
        compiler_params=pltpu.CompilerParams(
            collective_id=0, has_side_effects=True, vmem_limit_bytes=60 * 1024 * 1024
        ),
        name="fused",
    )(
        mixer_input, log_forget_total, mixer_gain[None], w_query, w_key.T, w_value.T, w_output,
        mixer_post_gain[None], expert_input, expert_ids.T, route_weight.T, expert_gain[None],
        w_gate[0], w_up[0], w_down[0], expert_post_gain[None],
    )


def solution(mesh):
    placed = (
        P("ep", None),
        P("tp", None),
        P(),
        P(None, "tp"),
        P(None, "tp"),
        P(None, "tp"),
        P(),
        P(),
        P("ep", None),
        P("ep", None),
        P("ep", None),
        P(),
        P("ep", None, "tp"),
        P("ep", None, "tp"),
        P("ep", "tp", None),
        P(),
    )
    return jax.shard_map(
        per_device,
        mesh=mesh,
        in_specs=placed,
        out_specs=(P(("ep", "tp"), None), P(("ep", "tp"), None)),
        check_vma=False,
    )
```

```python
import functools

import jax
import jax.numpy as jnp
from jax import lax
from jax.experimental import pallas as pl
from jax.experimental.pallas import tpu as pltpu
from jax.sharding import PartitionSpec as P

HD = 64
TOP_K = 2
ONES = 16
LOG2E = 1.4426950408889634
NEG_FILL = -1e30
NORM_EPS = 1e-06
MESH = pl.DeviceIdType.MESH
SOON = 5
LATER = 8


def norm_rows(values_in, gain_vec):
    widened = values_in.astype(jnp.float32)
    return (
        widened
        * lax.rsqrt(jnp.mean(widened * widened, axis=-1, keepdims=True) + NORM_EPS)
        * gain_vec
    )


def three_pieces(wide):
    high = wide.astype(jnp.bfloat16)
    rest = wide - high.astype(jnp.float32)
    middle = rest.astype(jnp.bfloat16)
    low = (rest - middle.astype(jnp.float32)).astype(jnp.bfloat16)
    return high, middle, low


def contract(a, b, left, right):
    return lax.dot_general(
        a, b, (((left,), (right,)), ((), ())), preferred_element_type=jnp.float32
    )


def flip(place, step, size):
    total = 0
    bit = 1
    while bit < size:
        total = total + lax.rem(place // bit + step // bit, 2) * bit
        bit *= 2
    return total


def fused_kernel(
    n_ep, x_hbm, gate_hbm, gain_hbm, wq_hbm, wk_hbm, wv_hbm, wo_hbm, post_hbm, xin_hbm,
    ids_hbm, share_hbm, egain_hbm, wg_hbm, wu_hbm, wd_hbm, epost_hbm,
    mixer_ref, expert_ref,
    gate_ref, gain_ref, post_ref, ids_ref, share_ref, egain_ref, epost_ref, x_v, wq_v, wkv_v, wo_v, xin_v, wgu_v, wd_v, out_rows, slots, product, arrived, summed,
    crossed, final, returned, weigh_v, kv_all, q_full, max_ref, acc_ref, mixed_v, heads_v,
    l_sem, ep_sem, x_sem, c_sem, d_sem, p_sem, r_sem, s_sem, b_sem, k_sem, f_sem, h_sem,
):
    own = lax.axis_index("ep")
    quarter = lax.axis_index("tp")
    across = lax.rem(quarter + 2, 4)
    beside = quarter + 1 - 2 * lax.rem(quarter, 2)
    diagonal = lax.rem(beside + 2, 4)
    column = lax.rem(own, 2)
    row = own // 2
    row_total = n_ep // 2
    partner = own + 1 - 2 * column
    heads, _, rows = q_full.shape
    token_rows = xin_v.shape[0]
    cap = out_rows.shape[1]
    width = out_rows.shape[2]
    units = wd_v.shape[0]

    def remote(source, target, sems, at_send, at_recv, axis, place):
        return pltpu.make_async_remote_copy(
            src_ref=source, dst_ref=target, send_sem=sems.at[0, at_send],
            recv_sem=sems.at[1, at_recv], device_id={axis: place}, device_id_type=MESH,
        )

    def local(index):
        pairs = (
            (ids_hbm, ids_ref),
            (xin_hbm.at[pl.ds(quarter * token_rows, token_rows)], xin_v),
            (egain_hbm, egain_ref),
            (share_hbm, share_ref),
            (x_hbm, x_v),
            (gain_hbm, gain_ref),
            (wk_hbm, wkv_v.at[0:HD]),
            (wv_hbm, wkv_v.at[HD : 2 * HD]),
            (wq_hbm, wq_v),
            (gate_hbm, gate_ref),
            (wg_hbm, wgu_v.at[:, 0:units]),
            (wu_hbm, wgu_v.at[:, units : 2 * units]),
            (wd_hbm, wd_v),
            (wo_hbm, wo_v),
            (post_hbm, post_ref),
            (epost_hbm, epost_ref),
        )
        return pltpu.make_async_copy(pairs[index][0], pairs[index][1], l_sem.at[index])

    for index in range(16):
        local(index).start()
    barrier = pltpu.get_barrier_semaphore()
    for axis, size in (("ep", n_ep), ("tp", 4)):
        place = lax.axis_index(axis)
        for step in range(1, size):
            pl.semaphore_signal(
                barrier, inc=1, device_id={axis: lax.rem(place + step, size)},
                device_id_type=MESH,
            )

    def ep_copy(source, place):
        return remote(
            out_rows.at[place], slots.at[quarter, source], ep_sem, place, source, "ep", place
        )

    def to_across(source):
        held = slots.at[quarter, source]
        return remote(held, held, x_sem, source, source, "tp", across)

    def from_across(source):
        held = slots.at[across, source]
        return remote(held, held, x_sem, source, source, "tp", across)

    def to_beside(source):
        held = slots.at[quarter, source]
        return remote(held, held, c_sem, source, source, "tp", beside)

    def from_beside(source):
        held = slots.at[beside, source]
        return remote(held, held, c_sem, source, source, "tp", beside)

    def second(source):
        held = slots.at[across, source]
        return remote(held, held, d_sem, source, source, "tp", beside)

    def from_second(source):
        held = slots.at[diagonal, source]
        return remote(held, held, d_sem, source, source, "tp", beside)

    def near(j):
        return remote(product.at[beside, j], arrived.at[0, j], p_sem, j, j, "tp", beside)

    def far(j):
        return remote(product.at[diagonal, j], arrived.at[1, j], r_sem, j, j, "tp", beside)

    def cross(j):
        return remote(summed.at[j], crossed.at[j], s_sem, j, j, "tp", across)

    def home(j, source):
        return remote(final.at[j], returned.at[source], b_sem, j, source, "ep", j)

    def chain(source, place):
        return remote(kv_all.at[source], kv_all.at[source], k_sem, source, source, "ep", place)

    def hand(source):
        return remote(kv_all.at[source], kv_all.at[source], f_sem, source, source, "ep", partner)

    def heads_copy(step):
        place = lax.rem(quarter + step, 4)
        return remote(mixed_v.at[place], heads_v.at[quarter], h_sem, step, step, "tp", place)

    def peer(step):
        return flip(own, step, n_ep)

    def own_part(wide):
        part = 0
        for k in range(4):
            chosen = (quarter == k).astype(wide.dtype)
            part = part + wide[:, k * token_rows : (k + 1) * token_rows] * chosen
        return part

    local(0).wait()
    ids = own_part(ids_ref[...])
    expert = lax.broadcasted_iota(jnp.int32, (n_ep, token_rows), 0)
    first_is = (expert == ids[0:1]).astype(jnp.float32)
    second_is = (expert == ids[1:2]).astype(jnp.float32)
    named = (first_is + second_is).astype(jnp.bfloat16)
    earlier = (
        lax.broadcasted_iota(jnp.int32, (token_rows, token_rows), 0)
        < lax.broadcasted_iota(jnp.int32, (token_rows, token_rows), 1)
    ).astype(jnp.bfloat16)
    before = jnp.dot(named, earlier, preferred_element_type=jnp.float32).astype(jnp.bfloat16)
    total = n_ep * cap
    at_row = lax.broadcasted_iota(jnp.int32, (total, n_ep), 0)
    low_row = lax.broadcasted_iota(jnp.int32, (total, n_ep), 1) * cap
    spread = ((at_row >= low_row) & (at_row < low_row + cap)).astype(jnp.bfloat16)
    rank = (lax.broadcasted_iota(jnp.int32, (total, token_rows), 0) & (cap - 1)).astype(
        jnp.float32
    )
    here = jnp.dot(spread, before, preferred_element_type=jnp.float32) == rank
    sel = jnp.where(here, jnp.dot(spread, named, preferred_element_type=jnp.float32), 0.0)
    local(1).wait()
    local(2).wait()
    normed_m = norm_rows(xin_v[...], egain_ref[...]).astype(jnp.bfloat16)
    outgoing = jnp.dot(sel.astype(jnp.bfloat16), normed_m, preferred_element_type=jnp.float32)
    out_rows[...] = outgoing.astype(jnp.bfloat16).reshape(out_rows.shape)
    slots[quarter, own] = out_rows[own]
    pl.semaphore_wait(barrier, n_ep - 1 + 3)
    for step in range(1, SOON):
        ep_copy(own, peer(step)).start()
    to_across(own).start()
    to_beside(own).start()

    local(4).wait()
    local(5).wait()
    slab = min(64, rows)

    def norm_slab(index, carry):
        at = pl.ds(pl.multiple_of(index * slab, slab), slab)
        x_v[at] = norm_rows(x_v[at], gain_ref[...]).astype(jnp.bfloat16)
        return carry

    lax.fori_loop(0, rows // slab, norm_slab, 0)
    local(6).wait()
    local(7).wait()
    kv_all[own] = contract(x_v[...], wkv_v[...], 1, 1).astype(jnp.bfloat16)

    @pl.when(row + 1 < row_total)
    def _():
        chain(own, own + 2).start()

    @pl.when(column == 0)
    def _():
        hand(own).start()

    def send_rest(step, carry):
        ep_copy(own, peer(step)).start()
        return carry

    lax.fori_loop(SOON, n_ep, send_rest, 0)
    local(8).wait()
    queries = jnp.dot(x_v[...], wq_v[...], preferred_element_type=jnp.float32)
    queries = queries.astype(jnp.bfloat16).astype(jnp.float32).T * (LOG2E * HD ** (-0.5))
    piece_row = lax.broadcasted_iota(jnp.int32, (HD, rows), 0)
    for head in range(heads):
        wide = queries[head * HD : (head + 1) * HD]
        high = wide.astype(jnp.bfloat16)
        q_full[head, 0:HD] = high
        q_full[head, HD : 2 * HD] = jnp.zeros((HD, rows), jnp.bfloat16)
        q_full[head, 2 * HD : 3 * HD] = (wide - high.astype(jnp.float32)).astype(jnp.bfloat16)
        ones = (piece_row == head) | (piece_row == heads + head) | (piece_row == 2 * heads + head)
        q_full[head, 3 * HD : 4 * HD] = ones.astype(jnp.bfloat16)

    low_lane = lax.broadcasted_iota(jnp.int32, (n_ep, total), 0) * cap
    at_lane = lax.broadcasted_iota(jnp.int32, (n_ep, total), 1)
    spread_t = ((at_lane >= low_lane) & (at_lane < low_lane + cap)).astype(jnp.bfloat16)
    rank_t = (lax.broadcasted_iota(jnp.int32, (token_rows, total), 1) & (cap - 1)).astype(
        jnp.float32
    )
    here_t = contract(before, spread_t, 0, 0) == rank_t
    local(3).wait()
    shares = own_part(share_ref[...])
    weighed = first_is * shares[0:1] + second_is * shares[1:2]
    for index, piece in enumerate(three_pieces(weighed)):
        placed = jnp.where(here_t, contract(piece, spread_t, 0, 0), 0.0)
        weigh_v[index * token_rows : (index + 1) * token_rows] = placed.astype(jnp.bfloat16)

    max_ref[...] = jnp.full(max_ref.shape, NEG_FILL, jnp.float32)
    acc_ref[...] = jnp.zeros(acc_ref.shape, jnp.float32)

    def attend(index, diag):
        kv = kv_all[index]
        first = pl.multiple_of(index * rows, rows)
        pieces = three_pieces(gate_ref[:, pl.ds(first, rows)] * (-LOG2E))
        pieces = [piece.astype(jnp.float32) for piece in pieces]
        stacked = jnp.concatenate(
            [jnp.zeros((HD, rows), jnp.float32)]
            + pieces
            + [jnp.zeros((HD - 3 * heads, rows), jnp.float32)],
            axis=0,
        )
        lane = lax.broadcasted_iota(jnp.int32, kv.shape, 1)
        gated = jnp.where(lane < HD, kv, stacked.T.astype(jnp.bfloat16))
        keys = jnp.concatenate([kv, gated], axis=1)
        values = kv.T
        at = lax.broadcasted_iota(jnp.int32, values.shape, 0)
        values = jnp.where(at < HD, jnp.ones_like(values), values)[HD - ONES :]
        for head in range(heads):
            scores = jnp.dot(keys, q_full[head], preferred_element_type=jnp.float32)
            if diag:
                key = lax.broadcasted_iota(jnp.int32, scores.shape, 0)
                query = lax.broadcasted_iota(jnp.int32, scores.shape, 1)
                scores = jnp.where(key <= query, scores, NEG_FILL)
            old_max = max_ref[head]
            new_max = jnp.maximum(old_max, jnp.max(scores, axis=0, keepdims=True))
            shifted = jnp.exp2(scores - new_max).astype(jnp.bfloat16)
            acc_ref[head] = acc_ref[head] * jnp.exp2(old_max - new_max) + jnp.dot(
                values, shifted, preferred_element_type=jnp.float32
            )
            max_ref[head] = new_max

    for index in (9, 10, 11, 12):
        local(index).wait()

    def block_of(t):
        return own + lax.rem(t, 2) * (partner - own) - 2 * (t // 2)

    def pass_across(step):
        j = peer(step)
        far(j).wait_recv()
        pair = product[across, j].astype(jnp.float32) + arrived[1, j].astype(jnp.float32)
        summed[j] = pair.astype(jnp.bfloat16)
        cross(j).start()

    def finish(step):
        j = peer(step)
        near(j).wait_recv()
        cross(j).wait_recv()
        whole = product[quarter, j].astype(jnp.float32) + arrived[0, j].astype(jnp.float32)
        final[j] = (whole + crossed[j].astype(jnp.float32)).astype(jnp.bfloat16)

        @pl.when(step > 0)
        def _():
            home(j, own).start()

    half = n_ep // 2

    def cross_over(step):
        near_step = step - half + 1

        @pl.when((step >= half) & (step < n_ep))
        def _():
            pass_across(step)

        @pl.when((near_step >= 1) & (near_step < half))
        def _():
            pass_across(near_step)

        @pl.when(step == n_ep)
        def _():
            pass_across(0)

    def send_home(step):
        near_step = step - half + 1

        @pl.when((step >= half) & (step < n_ep))
        def _():
            finish(step)

        @pl.when((near_step >= 1) & (near_step < half))
        def _():
            finish(near_step)

        @pl.when(step == n_ep)
        def _():
            finish(0)

    def run(t, carry):
        @pl.when((t > 0) & (t < n_ep))
        def _():
            source = peer(t)
            ep_copy(source, source).wait_recv()
            to_across(source).start()
            to_beside(source).start()

        early = t - LATER + 2

        @pl.when((early > 0) & (lax.rem(early + n_ep, 2) == 0) & (early <= 2 * row))
        def _():
            source = own - early
            chain(source, own).wait_recv()
            hand(source).start()

            @pl.when(row + 1 < row_total)
            def _():
                chain(source, own + 2).start()

        @pl.when((t >= 2) & (t < n_ep + 2))
        def _():
            source = peer(t - 2)
            from_across(source).wait_recv()
            second(source).start()

        cross_over(t - 4)

        @pl.when((t >= 3) & (t < n_ep + 3))
        def _():
            source = peer(t - 3)
            from_beside(source).wait_recv()
            from_second(source).wait_recv()
            tokens = slots[:, source].reshape(4 * cap, width)
            both = jnp.dot(tokens, wgu_v[...], preferred_element_type=jnp.float32)
            gate_part = both[:, :units]
            hidden = gate_part / (1.0 + jnp.exp(-gate_part)) * both[:, units:]
            terms = jnp.dot(
                hidden.astype(jnp.bfloat16), wd_v[...], preferred_element_type=jnp.float32
            )
            product[:, source] = terms.astype(jnp.bfloat16).reshape(4, cap, width)
            far(source).start()
            near(source).start()

        @pl.when(t == 2)
        def _():
            attend(own, True)

        @pl.when((t > LATER) & (t < n_ep + LATER))
        def _():
            turn = t - LATER

            @pl.when((turn // 2 <= row) & ((turn > 1) | (column == 1)))
            def _():
                block = block_of(turn)

                @pl.when(lax.rem(turn, 2) == 1)
                def _():
                    hand(block).wait_recv()

                attend(block, False)

        send_home(t - 5)

        done = t - LATER - 2 * row

        @pl.when(done == 1)
        def _():
            parts = [acc_ref[head, ONES:] / acc_ref[head, 0:1] for head in range(heads)]
            mixed = jnp.concatenate(parts, axis=0).T.astype(jnp.bfloat16)
            mixed_v[...] = mixed.reshape(mixed_v.shape)
            for step in range(1, 4):
                heads_copy(step).start()
            heads_v[quarter] = mixed_v[quarter]

        @pl.when(t == n_ep + LATER)
        def _():
            for step in range(1, 4):
                heads_copy(step).wait()
            local(13).wait()
            local(14).wait()
            by_rows = jnp.concatenate([heads_v[k] for k in range(4)], axis=1)
            projected = jnp.dot(by_rows, wo_v[...], preferred_element_type=jnp.float32)
            mixer_ref[...] = norm_rows(projected, post_ref[...]).astype(jnp.bfloat16)

        return carry

    lax.fori_loop(0, n_ep + LATER + 1, run, 0)
    returned[own] = final[own]

    def come_home(step, carry):
        j = flip(own, step, n_ep)
        home(j, j).wait_recv()
        return carry

    lax.fori_loop(1, n_ep, come_home, 0)
    local(15).wait()
    rows_back = returned[...].reshape(total, width)
    picked = jnp.dot(weigh_v[...], rows_back, preferred_element_type=jnp.float32)
    combined = picked[:token_rows] + picked[token_rows : 2 * token_rows]
    combined = combined + picked[2 * token_rows :]
    expert_ref[...] = norm_rows(combined, epost_ref[...]).astype(jnp.bfloat16)

    def drain(step, carry):
        j = flip(own, step, n_ep)
        to_across(j).wait_send()
        to_beside(j).wait_send()
        second(j).wait_send()
        near(j).wait_send()
        far(j).wait_send()
        cross(j).wait_send()

        @pl.when(step > 0)
        def _():
            ep_copy(own, j).wait_send()
            home(j, own).wait_send()

        return carry

    lax.fori_loop(0, n_ep, drain, 0)

    def drain_kv(step, carry):
        source = own - 2 * step

        @pl.when((step <= row) & (row + 1 < row_total))
        def _():
            chain(source, own + 2).wait_send()

        @pl.when((step <= row) & ((step > 0) | (column == 0)))
        def _():
            hand(source).wait_send()

        return carry

    lax.fori_loop(0, row_total, drain_kv, 0)


def deliver_kernel(mixer_in, expert_in, mixer_out, expert_out):
    mixer_out[...] = mixer_in[...]
    expert_out[...] = expert_in[...]


def per_device(
    mixer_input, log_forget_total, mixer_gain, w_query, w_key, w_value, w_output,
    mixer_post_gain, expert_input, expert_ids, route_weight, expert_gain, w_gate, w_up,
    w_down, expert_post_gain,
):
    n_ep = lax.axis_size("ep")
    rows, width = mixer_input.shape
    head_columns = w_query.shape[1]
    heads = head_columns // HD
    token_rows = expert_input.shape[0] // 4
    cap = 2 * TOP_K * token_rows // n_ep
    units = w_gate.shape[2]
    out_columns = w_output.shape[0]
    half = jnp.bfloat16
    chunk = (n_ep, cap, width)
    pair = pltpu.SemaphoreType.DMA((2, n_ep))
    vmem = pl.BlockSpec(memory_space=pltpu.VMEM)
    far_memory = pl.BlockSpec(memory_space=pltpu.HBM)
    gains = pltpu.VMEM((1, width), jnp.float32)
    scratch = [
        pltpu.VMEM(log_forget_total.shape, jnp.float32),
        gains,
        gains,
        pltpu.VMEM((TOP_K, 4 * token_rows), jnp.int32),
        pltpu.VMEM((TOP_K, 4 * token_rows), jnp.float32),
        gains,
        gains,
        pltpu.VMEM((rows, width), half),
        pltpu.VMEM((width, head_columns), half),
        pltpu.VMEM((2 * HD, width), half),
        pltpu.VMEM((out_columns, width), half),
        pltpu.VMEM((token_rows, width), half),
        pltpu.VMEM((width, 2 * units), half),
        pltpu.VMEM((units, width), half),
        pltpu.VMEM(chunk, half),
        pltpu.VMEM((4,) + chunk, half),
        pltpu.VMEM((4,) + chunk, half),
        pltpu.VMEM((2,) + chunk, half),
        pltpu.VMEM(chunk, half),
        pltpu.VMEM(chunk, half),
        pltpu.VMEM(chunk, half),
        pltpu.VMEM(chunk, half),
        pltpu.VMEM((3 * token_rows, n_ep * cap), half),
        pltpu.VMEM((n_ep, rows, 2 * HD), half),
        pltpu.VMEM((heads, 4 * HD, rows), half),
        pltpu.VMEM((heads, 1, rows), jnp.float32),
        pltpu.VMEM((heads, HD + ONES, rows), jnp.float32),
        pltpu.VMEM((4, rows // 4, head_columns), half),
        pltpu.VMEM((4, rows // 4, head_columns), half),
        pltpu.SemaphoreType.DMA((16,)),
    ] + [pair] * 10 + [pltpu.SemaphoreType.DMA((2, 4))]
    results = pl.pallas_call(
        functools.partial(fused_kernel, n_ep),
        out_shape=(
            jax.ShapeDtypeStruct((rows // 4, width), half),
            jax.ShapeDtypeStruct((token_rows, width), half),
        ),
        in_specs=[far_memory] * 16,
        out_specs=(vmem, vmem),
        scratch_shapes=scratch,
        compiler_params=pltpu.CompilerParams(
            collective_id=0, has_side_effects=True, vmem_limit_bytes=60 * 1024 * 1024
        ),
        name="fused",
    )(
        mixer_input, log_forget_total, mixer_gain[None], w_query, w_key.T, w_value.T, w_output,
        mixer_post_gain[None], expert_input, expert_ids.T, route_weight.T, expert_gain[None],
        w_gate[0], w_up[0], w_down[0], expert_post_gain[None],
    )
    return pl.pallas_call(
        deliver_kernel,
        out_shape=tuple(jax.ShapeDtypeStruct(part.shape, half) for part in results),
        in_specs=[vmem, vmem],
        out_specs=(vmem, vmem),
        name="deliver",
    )(*results)


def solution(mesh):
    placed = (
        P("ep", None),
        P("tp", None),
        P(),
        P(None, "tp"),
        P(None, "tp"),
        P(None, "tp"),
        P(),
        P(),
        P("ep", None),
        P("ep", None),
        P("ep", None),
        P(),
        P("ep", None, "tp"),
        P("ep", None, "tp"),
        P("ep", "tp", None),
        P(),
    )
    return jax.shard_map(
        per_device,
        mesh=mesh,
        in_specs=placed,
        out_specs=(P(("ep", "tp"), None), P(("ep", "tp"), None)),
        check_vma=False,
    )
```

```python
import functools

import jax
import jax.numpy as jnp
from jax import lax
from jax.experimental import pallas as pl
from jax.experimental.pallas import tpu as pltpu
from jax.sharding import PartitionSpec as P

HD = 64
TOP_K = 2
ONES = 16
LOG2E = 1.4426950408889634
NEG_FILL = -1e30
NORM_EPS = 1e-06
MESH = pl.DeviceIdType.MESH
SOON = 5
LATER = 8


def norm_rows(values_in, gain_vec):
    widened = values_in.astype(jnp.float32)
    return (
        widened
        * lax.rsqrt(jnp.mean(widened * widened, axis=-1, keepdims=True) + NORM_EPS)
        * gain_vec
    )


def three_pieces(wide):
    high = wide.astype(jnp.bfloat16)
    rest = wide - high.astype(jnp.float32)
    middle = rest.astype(jnp.bfloat16)
    low = (rest - middle.astype(jnp.float32)).astype(jnp.bfloat16)
    return high, middle, low


def contract(a, b, left, right):
    return lax.dot_general(
        a, b, (((left,), (right,)), ((), ())), preferred_element_type=jnp.float32
    )


def flip(place, step, size):
    total = 0
    bit = 1
    while bit < size:
        total = total + lax.rem(place // bit + step // bit, 2) * bit
        bit *= 2
    return total


def fused_kernel(
    n_ep, x_hbm, gate_hbm, gain_hbm, wq_hbm, wk_hbm, wv_hbm, wo_hbm, post_hbm, xin_hbm,
    ids_hbm, share_hbm, egain_hbm, wg_hbm, wu_hbm, wd_hbm, epost_hbm,
    mixer_ref, expert_ref,
    gate_ref, gain_ref, post_ref, ids_ref, share_ref, egain_ref, epost_ref, x_v, wq_v, wkv_v, wo_v, xin_v, wgu_v, wd_v, out_rows, slots, product, arrived, summed,
    crossed, final, returned, weigh_v, kv_all, q_full, max_ref, acc_ref, mixed_v, heads_v,
    l_sem, ep_sem, x_sem, c_sem, d_sem, p_sem, r_sem, s_sem, b_sem, k_sem, f_sem, h_sem,
):
    own = lax.axis_index("ep")
    quarter = lax.axis_index("tp")
    across = lax.rem(quarter + 2, 4)
    beside = quarter + 1 - 2 * lax.rem(quarter, 2)
    diagonal = lax.rem(beside + 2, 4)
    column = lax.rem(own, 2)
    row = own // 2
    row_total = n_ep // 2
    partner = own + 1 - 2 * column
    heads, _, rows = q_full.shape
    token_rows = xin_v.shape[0]
    cap = out_rows.shape[1]
    width = out_rows.shape[2]
    units = wd_v.shape[0]

    def remote(source, target, sems, at_send, at_recv, axis, place):
        return pltpu.make_async_remote_copy(
            src_ref=source, dst_ref=target, send_sem=sems.at[0, at_send],
            recv_sem=sems.at[1, at_recv], device_id={axis: place}, device_id_type=MESH,
        )

    def local(index):
        pairs = (
            (ids_hbm, ids_ref),
            (xin_hbm.at[pl.ds(quarter * token_rows, token_rows)], xin_v),
            (egain_hbm, egain_ref),
            (share_hbm, share_ref),
            (x_hbm, x_v),
            (gain_hbm, gain_ref),
            (wk_hbm, wkv_v.at[0:HD]),
            (wv_hbm, wkv_v.at[HD : 2 * HD]),
            (wq_hbm, wq_v),
            (gate_hbm, gate_ref),
            (wg_hbm, wgu_v.at[:, 0:units]),
            (wu_hbm, wgu_v.at[:, units : 2 * units]),
            (wd_hbm, wd_v),
            (wo_hbm, wo_v),
            (post_hbm, post_ref),
            (epost_hbm, epost_ref),
        )
        return pltpu.make_async_copy(pairs[index][0], pairs[index][1], l_sem.at[index])

    for index in range(16):
        local(index).start()
    barrier = pltpu.get_barrier_semaphore()
    for axis, size in (("ep", n_ep), ("tp", 4)):
        place = lax.axis_index(axis)
        for step in range(1, size):
            pl.semaphore_signal(
                barrier, inc=1, device_id={axis: lax.rem(place + step, size)},
                device_id_type=MESH,
            )

    def ep_copy(source, place):
        return remote(
            out_rows.at[place], slots.at[quarter, source], ep_sem, place, source, "ep", place
        )

    def to_across(source):
        held = slots.at[quarter, source]
        return remote(held, held, x_sem, source, source, "tp", across)

    def from_across(source):
        held = slots.at[across, source]
        return remote(held, held, x_sem, source, source, "tp", across)

    def to_beside(source):
        held = slots.at[quarter, source]
        return remote(held, held, c_sem, source, source, "tp", beside)

    def from_beside(source):
        held = slots.at[beside, source]
        return remote(held, held, c_sem, source, source, "tp", beside)

    def second(source):
        held = slots.at[across, source]
        return remote(held, held, d_sem, source, source, "tp", beside)

    def from_second(source):
        held = slots.at[diagonal, source]
        return remote(held, held, d_sem, source, source, "tp", beside)

    def near(j):
        return remote(product.at[beside, j], arrived.at[0, j], p_sem, j, j, "tp", beside)

    def far(j):
        return remote(product.at[diagonal, j], arrived.at[1, j], r_sem, j, j, "tp", beside)

    def cross(j):
        return remote(summed.at[j], crossed.at[j], s_sem, j, j, "tp", across)

    def home(j, source):
        return remote(final.at[j], returned.at[source], b_sem, j, source, "ep", j)

    def chain(source, place):
        return remote(kv_all.at[source], kv_all.at[source], k_sem, source, source, "ep", place)

    def hand(source):
        return remote(kv_all.at[source], kv_all.at[source], f_sem, source, source, "ep", partner)

    def heads_copy(step):
        place = lax.rem(quarter + step, 4)
        return remote(mixed_v.at[place], heads_v.at[quarter], h_sem, step, step, "tp", place)

    def peer(step):
        return flip(own, step, n_ep)

    def own_part(wide):
        part = 0
        for k in range(4):
            chosen = (quarter == k).astype(wide.dtype)
            part = part + wide[:, k * token_rows : (k + 1) * token_rows] * chosen
        return part

    local(0).wait()
    ids = own_part(ids_ref[...])
    expert = lax.broadcasted_iota(jnp.int32, (n_ep, token_rows), 0)
    first_is = (expert == ids[0:1]).astype(jnp.float32)
    second_is = (expert == ids[1:2]).astype(jnp.float32)
    named = (first_is + second_is).astype(jnp.bfloat16)
    earlier = (
        lax.broadcasted_iota(jnp.int32, (token_rows, token_rows), 0)
        < lax.broadcasted_iota(jnp.int32, (token_rows, token_rows), 1)
    ).astype(jnp.bfloat16)
    before = jnp.dot(named, earlier, preferred_element_type=jnp.float32).astype(jnp.bfloat16)
    total = n_ep * cap
    at_row = lax.broadcasted_iota(jnp.int32, (total, n_ep), 0)
    low_row = lax.broadcasted_iota(jnp.int32, (total, n_ep), 1) * cap
    spread = ((at_row >= low_row) & (at_row < low_row + cap)).astype(jnp.bfloat16)
    rank = (lax.broadcasted_iota(jnp.int32, (total, token_rows), 0) & (cap - 1)).astype(
        jnp.float32
    )
    here = jnp.dot(spread, before, preferred_element_type=jnp.float32) == rank
    sel = jnp.where(here, jnp.dot(spread, named, preferred_element_type=jnp.float32), 0.0)
    local(1).wait()
    local(2).wait()
    normed_m = norm_rows(xin_v[...], egain_ref[...]).astype(jnp.bfloat16)
    outgoing = jnp.dot(sel.astype(jnp.bfloat16), normed_m, preferred_element_type=jnp.float32)
    out_rows[...] = outgoing.astype(jnp.bfloat16).reshape(out_rows.shape)
    slots[quarter, own] = out_rows[own]
    pl.semaphore_wait(barrier, n_ep - 1 + 3)
    for step in range(1, SOON):
        ep_copy(own, peer(step)).start()
    to_across(own).start()
    to_beside(own).start()

    local(4).wait()
    local(5).wait()
    slab = min(64, rows)

    def norm_slab(index, carry):
        at = pl.ds(pl.multiple_of(index * slab, slab), slab)
        x_v[at] = norm_rows(x_v[at], gain_ref[...]).astype(jnp.bfloat16)
        return carry

    lax.fori_loop(0, rows // slab, norm_slab, 0)
    local(6).wait()
    local(7).wait()
    kv_all[own] = contract(x_v[...], wkv_v[...], 1, 1).astype(jnp.bfloat16)

    @pl.when(row + 1 < row_total)
    def _():
        chain(own, own + 2).start()

    @pl.when(column == 0)
    def _():
        hand(own).start()

    def send_rest(step, carry):
        ep_copy(own, peer(step)).start()
        return carry

    lax.fori_loop(SOON, n_ep, send_rest, 0)
    local(8).wait()
    queries = jnp.dot(x_v[...], wq_v[...], preferred_element_type=jnp.float32)
    queries = queries.astype(jnp.bfloat16).astype(jnp.float32).T * (LOG2E * HD ** (-0.5))
    piece_row = lax.broadcasted_iota(jnp.int32, (HD, rows), 0)
    for head in range(heads):
        wide = queries[head * HD : (head + 1) * HD]
        high = wide.astype(jnp.bfloat16)
        q_full[head, 0:HD] = high
        q_full[head, HD : 2 * HD] = jnp.zeros((HD, rows), jnp.bfloat16)
        q_full[head, 2 * HD : 3 * HD] = (wide - high.astype(jnp.float32)).astype(jnp.bfloat16)
        ones = (piece_row == head) | (piece_row == heads + head) | (piece_row == 2 * heads + head)
        q_full[head, 3 * HD : 4 * HD] = ones.astype(jnp.bfloat16)

    low_lane = lax.broadcasted_iota(jnp.int32, (n_ep, total), 0) * cap
    at_lane = lax.broadcasted_iota(jnp.int32, (n_ep, total), 1)
    spread_t = ((at_lane >= low_lane) & (at_lane < low_lane + cap)).astype(jnp.bfloat16)
    rank_t = (lax.broadcasted_iota(jnp.int32, (token_rows, total), 1) & (cap - 1)).astype(
        jnp.float32
    )
    here_t = contract(before, spread_t, 0, 0) == rank_t
    local(3).wait()
    shares = own_part(share_ref[...])
    weighed = first_is * shares[0:1] + second_is * shares[1:2]
    for index, piece in enumerate(three_pieces(weighed)):
        placed = jnp.where(here_t, contract(piece, spread_t, 0, 0), 0.0)
        weigh_v[index * token_rows : (index + 1) * token_rows] = placed.astype(jnp.bfloat16)

    max_ref[...] = jnp.full(max_ref.shape, NEG_FILL, jnp.float32)
    acc_ref[...] = jnp.zeros(acc_ref.shape, jnp.float32)

    def attend(index, diag):
        kv = kv_all[index]
        first = pl.multiple_of(index * rows, rows)
        pieces = three_pieces(gate_ref[:, pl.ds(first, rows)] * (-LOG2E))
        pieces = [piece.astype(jnp.float32) for piece in pieces]
        stacked = jnp.concatenate(
            [jnp.zeros((HD, rows), jnp.float32)]
            + pieces
            + [jnp.zeros((HD - 3 * heads, rows), jnp.float32)],
            axis=0,
        )
        lane = lax.broadcasted_iota(jnp.int32, kv.shape, 1)
        gated = jnp.where(lane < HD, kv, stacked.T.astype(jnp.bfloat16))
        keys = jnp.concatenate([kv, gated], axis=1)
        values = kv.T
        at = lax.broadcasted_iota(jnp.int32, values.shape, 0)
        values = jnp.where(at < HD, jnp.ones_like(values), values)[HD - ONES :]
        for head in range(heads):
            scores = jnp.dot(keys, q_full[head], preferred_element_type=jnp.float32)
            if diag:
                key = lax.broadcasted_iota(jnp.int32, scores.shape, 0)
                query = lax.broadcasted_iota(jnp.int32, scores.shape, 1)
                scores = jnp.where(key <= query, scores, NEG_FILL)
            old_max = max_ref[head]
            new_max = jnp.maximum(old_max, jnp.max(scores, axis=0, keepdims=True))
            shifted = jnp.exp2(scores - new_max).astype(jnp.bfloat16)
            acc_ref[head] = acc_ref[head] * jnp.exp2(old_max - new_max) + jnp.dot(
                values, shifted, preferred_element_type=jnp.float32
            )
            max_ref[head] = new_max

    for index in (9, 10, 11, 12):
        local(index).wait()

    def block_of(t):
        return own + lax.rem(t, 2) * (partner - own) - 2 * (t // 2)

    def pass_across(step):
        j = peer(step)
        far(j).wait_recv()
        pair = product[across, j].astype(jnp.float32) + arrived[1, j].astype(jnp.float32)
        summed[j] = pair.astype(jnp.bfloat16)
        cross(j).start()

    def finish(step):
        j = peer(step)
        near(j).wait_recv()
        cross(j).wait_recv()
        whole = product[quarter, j].astype(jnp.float32) + arrived[0, j].astype(jnp.float32)
        final[j] = (whole + crossed[j].astype(jnp.float32)).astype(jnp.bfloat16)

        @pl.when(step > 0)
        def _():
            home(j, own).start()

    half = n_ep // 2

    def cross_over(step):
        near_step = step - half + 1

        @pl.when((step >= half) & (step < n_ep))
        def _():
            pass_across(step)

        @pl.when((near_step >= 1) & (near_step < half))
        def _():
            pass_across(near_step)

        @pl.when(step == n_ep)
        def _():
            pass_across(0)

    def send_home(step):
        near_step = step - half + 1

        @pl.when((step >= half) & (step < n_ep))
        def _():
            finish(step)

        @pl.when((near_step >= 1) & (near_step < half))
        def _():
            finish(near_step)

        @pl.when(step == n_ep)
        def _():
            finish(0)

    later = LATER

    def run(t, carry):
        @pl.when((t > 0) & (t < n_ep))
        def _():
            source = peer(t)
            ep_copy(source, source).wait_recv()
            to_across(source).start()
            to_beside(source).start()

        early = t - later + 2

        @pl.when((early > 0) & (lax.rem(early + n_ep, 2) == 0) & (early <= 2 * row))
        def _():
            source = own - early
            chain(source, own).wait_recv()
            hand(source).start()

            @pl.when(row + 1 < row_total)
            def _():
                chain(source, own + 2).start()

        @pl.when((t >= 2) & (t < n_ep + 2))
        def _():
            source = peer(t - 2)
            from_across(source).wait_recv()
            second(source).start()

        cross_over(t - 4)

        @pl.when((t >= 3) & (t < n_ep + 3))
        def _():
            source = peer(t - 3)
            from_beside(source).wait_recv()
            from_second(source).wait_recv()
            tokens = slots[:, source].reshape(4 * cap, width)
            both = jnp.dot(tokens, wgu_v[...], preferred_element_type=jnp.float32)
            gate_part = both[:, :units]
            hidden = gate_part / (1.0 + jnp.exp(-gate_part)) * both[:, units:]
            terms = jnp.dot(
                hidden.astype(jnp.bfloat16), wd_v[...], preferred_element_type=jnp.float32
            )
            product[:, source] = terms.astype(jnp.bfloat16).reshape(4, cap, width)
            far(source).start()
            near(source).start()

        @pl.when(t == 1)
        def _():
            attend(own, True)

        @pl.when((t > later) & (t < n_ep + later))
        def _():
            turn = t - later

            @pl.when((turn // 2 <= row) & ((turn > 1) | (column == 1)))
            def _():
                block = block_of(turn)

                @pl.when(lax.rem(turn, 2) == 1)
                def _():
                    hand(block).wait_recv()

                attend(block, False)

        send_home(t - 5)

        settled = n_ep + 4
        ready = later + 2 * row + 1

        @pl.when(((t == ready) & (ready >= settled)) | ((t == settled) & (ready < settled)))
        def _():
            parts = [acc_ref[head, ONES:] / acc_ref[head, 0:1] for head in range(heads)]
            mixed = jnp.concatenate(parts, axis=0).T.astype(jnp.bfloat16)
            mixed_v[...] = mixed.reshape(mixed_v.shape)
            for step in range(1, 4):
                heads_copy(step).start()
            heads_v[quarter] = mixed_v[quarter]

        @pl.when(t == n_ep + LATER)
        def _():
            for step in range(1, 4):
                heads_copy(step).wait()
            local(13).wait()
            local(14).wait()
            by_rows = jnp.concatenate([heads_v[k] for k in range(4)], axis=1)
            projected = jnp.dot(by_rows, wo_v[...], preferred_element_type=jnp.float32)
            mixer_ref[...] = norm_rows(projected, post_ref[...]).astype(jnp.bfloat16)

        return carry

    lax.fori_loop(0, n_ep + LATER + 1, run, 0)
    returned[own] = final[own]

    def come_home(step, carry):
        j = flip(own, step, n_ep)
        home(j, j).wait_recv()
        return carry

    lax.fori_loop(1, n_ep, come_home, 0)
    local(15).wait()
    rows_back = returned[...].reshape(total, width)
    picked = jnp.dot(weigh_v[...], rows_back, preferred_element_type=jnp.float32)
    combined = picked[:token_rows] + picked[token_rows : 2 * token_rows]
    combined = combined + picked[2 * token_rows :]
    expert_ref[...] = norm_rows(combined, epost_ref[...]).astype(jnp.bfloat16)

    def drain(step, carry):
        j = flip(own, step, n_ep)
        to_across(j).wait_send()
        to_beside(j).wait_send()
        second(j).wait_send()
        near(j).wait_send()
        far(j).wait_send()
        cross(j).wait_send()

        @pl.when(step > 0)
        def _():
            ep_copy(own, j).wait_send()
            home(j, own).wait_send()

        return carry

    lax.fori_loop(0, n_ep, drain, 0)

    def drain_kv(step, carry):
        source = own - 2 * step

        @pl.when((step <= row) & (row + 1 < row_total))
        def _():
            chain(source, own + 2).wait_send()

        @pl.when((step <= row) & ((step > 0) | (column == 0)))
        def _():
            hand(source).wait_send()

        return carry

    lax.fori_loop(0, row_total, drain_kv, 0)


def deliver_kernel(mixer_in, expert_in, mixer_out, expert_out, mixer_v, expert_v, sems):
    taken = (
        pltpu.make_async_copy(mixer_in, mixer_v, sems.at[0]),
        pltpu.make_async_copy(expert_in, expert_v, sems.at[1]),
    )
    given = (
        pltpu.make_async_copy(mixer_v, mixer_out, sems.at[2]),
        pltpu.make_async_copy(expert_v, expert_out, sems.at[3]),
    )
    for copy in taken:
        copy.start()
    for arrival, departure in zip(taken, given):
        arrival.wait()
        departure.start()
    for copy in given:
        copy.wait()


def per_device(
    mixer_input, log_forget_total, mixer_gain, w_query, w_key, w_value, w_output,
    mixer_post_gain, expert_input, expert_ids, route_weight, expert_gain, w_gate, w_up,
    w_down, expert_post_gain,
):
    n_ep = lax.axis_size("ep")
    rows, width = mixer_input.shape
    head_columns = w_query.shape[1]
    heads = head_columns // HD
    token_rows = expert_input.shape[0] // 4
    cap = 2 * TOP_K * token_rows // n_ep
    units = w_gate.shape[2]
    out_columns = w_output.shape[0]
    half = jnp.bfloat16
    chunk = (n_ep, cap, width)
    pair = pltpu.SemaphoreType.DMA((2, n_ep))
    vmem = pl.BlockSpec(memory_space=pltpu.VMEM)
    far_memory = pl.BlockSpec(memory_space=pltpu.HBM)
    gains = pltpu.VMEM((1, width), jnp.float32)
    scratch = [
        pltpu.VMEM(log_forget_total.shape, jnp.float32),
        gains,
        gains,
        pltpu.VMEM((TOP_K, 4 * token_rows), jnp.int32),
        pltpu.VMEM((TOP_K, 4 * token_rows), jnp.float32),
        gains,
        gains,
        pltpu.VMEM((rows, width), half),
        pltpu.VMEM((width, head_columns), half),
        pltpu.VMEM((2 * HD, width), half),
        pltpu.VMEM((out_columns, width), half),
        pltpu.VMEM((token_rows, width), half),
        pltpu.VMEM((width, 2 * units), half),
        pltpu.VMEM((units, width), half),
        pltpu.VMEM(chunk, half),
        pltpu.VMEM((4,) + chunk, half),
        pltpu.VMEM((4,) + chunk, half),
        pltpu.VMEM((2,) + chunk, half),
        pltpu.VMEM(chunk, half),
        pltpu.VMEM(chunk, half),
        pltpu.VMEM(chunk, half),
        pltpu.VMEM(chunk, half),
        pltpu.VMEM((3 * token_rows, n_ep * cap), half),
        pltpu.VMEM((n_ep, rows, 2 * HD), half),
        pltpu.VMEM((heads, 4 * HD, rows), half),
        pltpu.VMEM((heads, 1, rows), jnp.float32),
        pltpu.VMEM((heads, HD + ONES, rows), jnp.float32),
        pltpu.VMEM((4, rows // 4, head_columns), half),
        pltpu.VMEM((4, rows // 4, head_columns), half),
        pltpu.SemaphoreType.DMA((16,)),
    ] + [pair] * 10 + [pltpu.SemaphoreType.DMA((2, 4))]
    results = pl.pallas_call(
        functools.partial(fused_kernel, n_ep),
        out_shape=(
            jax.ShapeDtypeStruct((rows // 4, width), half),
            jax.ShapeDtypeStruct((token_rows, width), half),
        ),
        in_specs=[far_memory] * 16,
        out_specs=(vmem, vmem),
        scratch_shapes=scratch,
        compiler_params=pltpu.CompilerParams(
            collective_id=0, has_side_effects=True, vmem_limit_bytes=60 * 1024 * 1024
        ),
        name="fused",
    )(
        mixer_input, log_forget_total, mixer_gain[None], w_query, w_key.T, w_value.T, w_output,
        mixer_post_gain[None], expert_input, expert_ids.T, route_weight.T, expert_gain[None],
        w_gate[0], w_up[0], w_down[0], expert_post_gain[None],
    )
    return pl.pallas_call(
        deliver_kernel,
        out_shape=tuple(jax.ShapeDtypeStruct(part.shape, half) for part in results),
        in_specs=[far_memory] * 2,
        out_specs=(far_memory,) * 2,
        scratch_shapes=[pltpu.VMEM(part.shape, half) for part in results]
        + [pltpu.SemaphoreType.DMA((4,))],
        name="deliver",
    )(*results)


def solution(mesh):
    placed = (
        P("ep", None),
        P("tp", None),
        P(),
        P(None, "tp"),
        P(None, "tp"),
        P(None, "tp"),
        P(),
        P(),
        P("ep", None),
        P("ep", None),
        P("ep", None),
        P(),
        P("ep", None, "tp"),
        P("ep", None, "tp"),
        P("ep", "tp", None),
        P(),
    )
    return jax.shard_map(
        per_device,
        mesh=mesh,
        in_specs=placed,
        out_specs=(P(("ep", "tp"), None), P(("ep", "tp"), None)),
        check_vma=False,
    )
```
